32 devices in a mesh: kv: 8 (over z, y), tp: 4 (over x, core).
Axes of the slice: x: 2, y: 2, z: 4, core: 2. Of those that a mesh axis runs over, the one named last changes fastest.
Arguments:
- queries: bfloat16 [6144, 2048], P('kv', 'tp'), may hold values from -6 to 6
- keys_values: bfloat16 [6144, 1024], P('kv', 'tp'), may hold values from -6 to 6
- log_sums: float32 [6144, 32], P('kv', 'tp'), may hold values from 6.5 to 7.5
- out_grad: bfloat16 [6144, 2048], P('kv', 'tp'), may hold values from -96 to 96
- inputs: bfloat16 [6144, 4096], P('kv'), may hold values from -0.046875 to 0.046875
- chosen: int32 [48, 16], P('kv'), may hold values from -1 to 95, as said below
Outputs:
- query_grad: bfloat16 [6144, 2048], P('kv', 'tp')
- kv_grad: float32 [6144, 1024], P('kv', 'tp')
- weight_grad: float32 [4096, 2048], P('kv', 'tp')
The draws below stay inside these ranges and needn't reach their ends.
Inputs may be any that keep to these rules, and one draw needn't show every extreme that they name: `chosen`: each row names distinct key blocks, none starting after the last position of that row's query block, and -1 in unused entries; at least half of 16 blocks are named where that many are allowed. From the query blocks of one index of kv, at most 6 distinct blocks of the 768 positions of any one index are named, and this most is reached on every index.
All inputs are finite; a program needn't handle non-finite values.
Results may differ from the reference program's by a relative error of at most 0.0051.
Values may be sent and summed in bfloat16 or wider, within the bound.
A program may use at most 128 MiB of HBM per device.

```python
import jax
import jax.numpy as jnp
from jax import lax

D = 4096
H = 32
KVH = 8
DH = 64
BLK = 64
QB = 128
NSEL = 16
TOK_DEV = 768
TOKENS = 6144


def draw_chosen(key, part):
    device_count = TOKENS // TOK_DEV
    query_per = TOK_DEV // QB
    block_per = TOK_DEV // BLK
    block_total = TOKENS // BLK
    query_total = TOKENS // QB
    capacity = block_per // 2
    key_order, key_pop, key_jitter, key_count = jax.random.split(key, 4)
    order_keys = jax.random.randint(key_order, (device_count, device_count, block_per), 0, 1 << 16) * block_per + jnp.arange(block_per, dtype=jnp.int32)
    order_rank = jnp.argsort(jnp.argsort(order_keys, axis=-1, stable=True), axis=-1, stable=True)
    allowed = order_rank < capacity
    popular = jax.random.randint(key_pop, (device_count,), 0, 4)
    jitter = jax.random.randint(key_jitter, (query_total, block_total), 0, 1024)
    counts = jax.random.randint(key_count, (query_total,), NSEL // 2, NSEL + 1)
    block_ids = jnp.arange(block_total, dtype=jnp.int32)
    owner_dev = block_ids // block_per
    within = block_ids % block_per
    query_ids = jnp.arange(query_total, dtype=jnp.int32)
    device = query_ids // query_per
    local_blk = query_ids % query_per
    allow_rows = allowed[device[:, None], owner_dev[None, :], within[None, :]]
    first_rank = order_rank[device[:, None], owner_dev[None, :], within[None, :]] == 0
    causal = (block_ids * BLK)[None, :] <= (query_ids * QB + QB - 1)[:, None]
    eligible = allow_rows & causal & (owner_dev[None, :] <= device[:, None])
    last_block = (local_blk == query_per - 1)[:, None]
    own_dev = owner_dev[None, :] == device[:, None]
    before_dev = owner_dev[None, :] == device[:, None] - 1
    half_dev = owner_dev[None, :] == device[:, None] - device_count // 2
    forced = last_block & eligible & (own_dev | first_rank & (before_dev | half_dev))
    block_score = jitter + popular[owner_dev][None, :] * 1024 + forced.astype(jnp.int32) * 8192
    block_score = jnp.where(eligible, block_score, -1)
    composite = block_score * block_total + block_ids[None, :]
    top_values, top_blocks = lax.top_k(composite, NSEL)
    listed = (jnp.arange(NSEL, dtype=jnp.int32)[None, :] < counts[:, None]) & (top_values >= 0)
    return jnp.where(listed, top_blocks, -1).astype(jnp.int32)


def with_spikes(entries, key, source, target, blocks, factor):
    def block_of(dim):
        return (jnp.arange(entries.shape[dim]) // (entries.shape[dim] // blocks)).reshape((-1,) + (1,) * (entries.ndim - 1 - dim))

    near = jax.random.permutation(key, blocks)[block_of(target)]
    far = (block_of(target) + blocks // 2) % blocks
    return jnp.where((block_of(source) == near) | (block_of(source) == far), factor * entries, entries)


def block_scale(rng, shape, cuts, smallest, top_value):
    gain = 1.0
    for axis_at, shards_of in cuts:
        steps = jax.random.uniform(jax.random.fold_in(jax.random.fold_in(rng, 6), axis_at), (shards_of,), jnp.float32, smallest / len(cuts), top_value / len(cuts))
        gain = gain * jnp.repeat(jnp.exp(steps), shape[axis_at] // shards_of).reshape((-1,) + (1,) * (len(shape) - 1 - axis_at))
    return gain


def normal_values(own_key, extent, width, reach, cuts=(), kind=jnp.bfloat16):
    result = jax.random.normal(own_key, extent, jnp.float32) * width
    if len(cuts) > 0:
        result = block_scale(own_key, extent, cuts, -0.22, 0.18) * result
    return jnp.clip(result, min=-reach, max=reach).astype(kind)


def gaussian_with(rng, extent, spread, bound, shards, heavy, kind=jnp.bfloat16):
    values = spread * jax.random.normal(rng, extent, jnp.float32)
    if shards:
        values = values * block_scale(rng, extent, shards, -0.22, 0.18)
    return jnp.clip(with_spikes(values, jax.random.fold_in(rng, 3), *heavy), -bound, bound).astype(kind)


def setup_inputs(seed: int = 0) -> dict:
    key_list = jax.random.split(jax.random.key(seed), 7)
    return {
        "queries": normal_values(key_list[0], (TOKENS, H * DH), 1.0, 6.0, ((0, 8), (1, 4))),
        "keys_values": normal_values(key_list[1], (TOKENS, 2 * KVH * DH), 1.0, 6.0, ((0, 8), (1, 4))),
        "log_sums": jnp.clip(6.5 + 1.0 * jax.random.uniform(key_list[2], (TOKENS, H), jnp.float32) ** block_scale(key_list[2], (TOKENS, H), ((0, 8), (1, 4)), -0.2, 0.2), 6.5, 7.5),
        "out_grad": normal_values(key_list[3], (TOKENS, H * DH), 16.0, 96.0, ((0, 8), (1, 4))),
        "inputs": gaussian_with(key_list[4], (TOKENS, D), 0.0078125, 0.046875, ((0, 8),), (0, 1, 8, 2.0)),
        "chosen": draw_chosen(jax.random.fold_in(key_list[6], 71), 0),
    }


def reference(queries, keys_values, log_sums, out_grad, inputs, chosen):
    score_scale = DH ** -0.5
    group_size = H // KVH
    block_total = TOKENS // BLK
    row_width = 2 * KVH * DH
    kv_blocks = keys_values.reshape(block_total, BLK, KVH, 2, DH)

    def one_block(grad_table, block_index):
        row_start = block_index * QB
        query_blk = lax.dynamic_slice_in_dim(queries, row_start, QB, 0).astype(jnp.float32).reshape(QB, KVH, group_size, DH)
        grad_blk = lax.dynamic_slice_in_dim(out_grad, row_start, QB, 0).astype(jnp.float32).reshape(QB, KVH, group_size, DH)
        sums_blk = lax.dynamic_slice_in_dim(log_sums, row_start, QB, 0).reshape(QB, KVH, group_size)
        chosen_row = lax.dynamic_index_in_dim(chosen, block_index, 0, keepdims=False)
        present = chosen_row >= 0
        safe_row = jnp.maximum(chosen_row, 0).astype(jnp.int32)
        picked = kv_blocks[safe_row].astype(jnp.float32)
        key_blk = picked[:, :, :, 0, :].reshape(NSEL * BLK, KVH, DH)
        value_blk = picked[:, :, :, 1, :].reshape(NSEL * BLK, KVH, DH)
        key_pos = (safe_row[:, None] * BLK + jnp.arange(BLK, dtype=jnp.int32)[None, :]).reshape(-1)
        key_live = jnp.repeat(present, BLK)
        query_pos = row_start + jnp.arange(QB, dtype=jnp.int32)
        visible = key_live[None, :] & (key_pos[None, :] <= query_pos[:, None])
        scores = jnp.einsum('qhgd,nhd->qhgn', query_blk, key_blk) * score_scale
        attn_prob = jnp.where(visible[:, None, None, :], jnp.exp(scores - sums_blk[..., None]), jnp.float32(0.0))
        prob_round = lax.optimization_barrier(attn_prob.astype(jnp.bfloat16)).astype(jnp.float32)
        output = jnp.einsum('qhgn,nhd->qhgd', prob_round, value_blk)
        delta_row = jnp.sum(grad_blk * output, axis=-1)
        prob_grad = jnp.einsum('qhgd,nhd->qhgn', grad_blk, value_blk)
        score_grad = attn_prob * (prob_grad - delta_row[..., None])
        score_round = lax.optimization_barrier(score_grad.astype(jnp.bfloat16)).astype(jnp.float32)
        query_part = (score_scale * jnp.einsum('qhgn,nhd->qhgd', score_round, key_blk)).astype(jnp.bfloat16)
        key_part = score_scale * jnp.einsum('qhgn,qhgd->nhd', score_round, query_blk)
        value_part = jnp.einsum('qhgn,qhgd->nhd', prob_round, grad_blk)
        both_parts = jnp.stack([key_part, value_part], axis=2).reshape(NSEL, BLK, row_width)
        grad_table = grad_table.at[safe_row].add(both_parts)
        return grad_table, query_part.reshape(QB, H * DH)

    start_table = jnp.zeros((block_total, BLK, row_width), jnp.float32)
    grad_table, query_parts = lax.scan(one_block, start_table, jnp.arange(TOKENS // QB, dtype=jnp.int32))
    query_grad = query_parts.reshape(TOKENS, H * DH)
    kv_grad = grad_table.reshape(TOKENS, row_width)
    weight_grad = jnp.dot(inputs.T, query_grad, preferred_element_type=jnp.float32)
    return query_grad, kv_grad, weight_grad
```

```python
import functools

import jax
import jax.numpy as jnp
from jax import lax
from jax.experimental import pallas as pl
from jax.experimental.pallas import tpu as pltpu
from jax.sharding import PartitionSpec as P

DH = 64
BLK = 64
QB = 128
NSEL = 16
CHUNK = 4
SCALE = DH ** (-0.5)
MESH = pl.DeviceIdType.MESH
SUBS = 4


def whole(n, kv_heads, group, tok, start_ref, first_ref, pos_ref, q_ref, do_ref, ls_ref, kv_hbm, inp_hbm,
          dq_ref, kvg_ref, wg_ref, *scratch):
    it = iter(scratch)
    tabs = [next(it) for _ in range(kv_heads)]
    qts = [next(it) for _ in range(kv_heads)]
    owns = [next(it) for _ in range(kv_heads)]
    ysend = [next(it) for _ in range(kv_heads)]
    yrecv = [next(it) for _ in range(kv_heads)]
    zsend = [next(it) for _ in range(kv_heads)]
    zrecv = [next(it) for _ in range(kv_heads)]
    rsend = [next(it) for _ in range(kv_heads)]
    rrecv = [next(it) for _ in range(kv_heads)]
    inp, w1, kv_scr, p_scr, dp_scr, a_scr, both_scr = [next(it) for _ in range(7)]
    (inp_sem, own_sem, fz_s, fy_s, f_r, gy_s, gy_r, gz_s, gz_r, r_s, r_r) = [next(it) for _ in range(11)]

    rows_n = n // 2
    nqb = tok // QB
    nblk = tok // BLK
    lanes = group * QB
    width = group * DH
    sub_w = width // SUBS
    me = lax.axis_index("kv")
    r, c = me // 2, me % 2
    partner = 2 * r + 1 - c
    up, down = me + 2, me - 2
    has_up, has_down = r < rows_n - 1, r > 0

    def at_pos(p):
        p = lax.rem(p + 2 * n, n)
        return jnp.where(p < rows_n, 2 * p, 2 * (n - 1 - p) + 1)

    pos_me = jnp.where(c == 0, r, n - 1 - r)
    ring_to = (at_pos(pos_me + 1), at_pos(pos_me - 1))

    barrier = pltpu.get_barrier_semaphore()
    pl.semaphore_signal(barrier, inc=1, device_id={"kv": partner}, device_id_type=MESH)

    @pl.when(has_up)
    def _():
        pl.semaphore_signal(barrier, inc=1, device_id={"kv": up}, device_id_type=MESH)

    @pl.when(has_down)
    def _():
        pl.semaphore_signal(barrier, inc=1, device_id={"kv": down}, device_id_type=MESH)

    own_rows = pl.ds(me * nblk, nblk)
    own_cp = [
        pltpu.make_async_copy(kv_hbm.at[:, :, h * 2 * DH:(h + 1) * 2 * DH], tabs[h].at[own_rows], own_sem.at[h])
        for h in range(kv_heads)
    ]
    for cp in own_cp:
        cp.start()
    drow = inp_hbm.shape[1] // n
    inp_cp = [
        pltpu.make_async_copy(inp_hbm.at[:, i * drow:(i + 1) * drow], inp.at[i], inp_sem.at[i]) for i in range(n)
    ]
    for cp in inp_cp:
        cp.start()
    w1[...] = jnp.zeros_like(w1)
    both_scr[nqb * NSEL] = jnp.zeros((BLK, 2 * DH), jnp.float32)
    for cp in own_cp:
        cp.wait()
    pl.semaphore_wait(barrier, 1 + has_up.astype(jnp.int32) + has_down.astype(jnp.int32))

    def fetch(h, owner, sems, slot, target):
        rows = pl.ds(owner * nblk, nblk)
        return pltpu.make_async_remote_copy(
            src_ref=tabs[h].at[rows], dst_ref=tabs[h].at[rows], send_sem=sems.at[h, slot],
            recv_sem=f_r.at[h, owner], device_id={"kv": target}, device_id_type=MESH)

    def forward(h, k):
        owner = 2 * (r - k) + c

        @pl.when(r >= k)
        def _():
            if k > 0:
                fetch(h, owner, fz_s, k, partner).wait_recv()

            @pl.when(has_up)
            def _():
                fetch(h, owner, fz_s, k, up).start()

            @pl.when((c == 0) if k == 0 else (c >= 0))
            def _():
                fetch(h, owner, fy_s, k, partner).start()

    def arrived(h):
        for k in range(rows_n):
            @pl.when((r >= k) if k > 0 else (c == 1))
            def _():
                fetch(h, 2 * (r - k) + 1 - c, fy_s, k, partner).wait_recv()

    def attend(h, qb):
        tab = tabs[h]
        qrow = pl.ds(pl.multiple_of(qb * QB, QB), QB)
        cols = slice(h * width, (h + 1) * width)
        q_t = (q_ref[qrow, cols].astype(jnp.float32) * SCALE).T.astype(jnp.bfloat16)
        do_t = do_ref[qrow, cols].astype(jnp.float32).T.astype(jnp.bfloat16)
        for g in range(group):
            w1[:DH, g * QB:(g + 1) * QB] = q_t[g * DH:(g + 1) * DH]
            w1[DH:, lanes + g * QB:lanes + (g + 1) * QB] = do_t[g * DH:(g + 1) * DH]
        for j in range(NSEL):
            kv_scr[j * BLK:(j + 1) * BLK, :] = tab[start_ref[qb, j]]
        rows = CHUNK * BLK
        lane = lax.broadcasted_iota(jnp.int32, (1, lanes), 1)
        qpos = (me * nqb + qb) * QB + lax.rem(lane, QB)
        within = lax.broadcasted_iota(jnp.int32, (BLK, lanes), 0)
        sums = ls_ref[h * nqb + qb]
        delta = jnp.zeros((1, lanes), jnp.float32)
        for ch in range(NSEL // CHUNK):
            kv = kv_scr[ch * rows:(ch + 1) * rows, :]
            scores = jnp.dot(kv, w1[:, :lanes], preferred_element_type=jnp.float32)
            grads = jnp.dot(kv, w1[:, lanes:], preferred_element_type=jnp.float32)
            for i in range(CHUNK):
                last = qpos - first_ref[qb, ch * CHUNK + i]
                here = slice(i * BLK, (i + 1) * BLK)
                there = slice(ch * rows + i * BLK, ch * rows + (i + 1) * BLK)
                prob = jnp.where(within <= last, jnp.exp(scores[here] - sums), jnp.float32(0.0))
                rounded = prob.astype(jnp.bfloat16)
                delta += jnp.sum(rounded.astype(jnp.float32) * grads[here], axis=0, keepdims=True)
                p_scr[there, :] = prob
                dp_scr[there, :] = grads[here]
                a_scr[there, lanes:] = rounded
        for ch in range(NSEL // CHUNK):
            there = slice(ch * rows, (ch + 1) * rows)
            a_scr[there, :lanes] = (p_scr[there, :] * (dp_scr[there, :] - delta)).astype(jnp.bfloat16)
            both_scr[pl.ds(qb * NSEL + ch * CHUNK, CHUNK)] = lax.dot_general(
                a_scr[there, :], w1[...], (((1,), (1,)), ((), ())), preferred_element_type=jnp.float32
            ).reshape(CHUNK, BLK, 2 * DH)
        dq_t = jnp.dot(kv_scr[...].T, a_scr[:, :lanes], preferred_element_type=jnp.float32)[:DH] * SCALE
        stacked = jnp.concatenate([dq_t[:, g * QB:(g + 1) * QB] for g in range(group)], axis=0)
        qts[h][qb] = stacked.astype(jnp.bfloat16)
        dq_ref[qrow, cols] = stacked.T.astype(jnp.bfloat16)

    def block_sum(block):
        total = None
        for qb in range(nqb):
            part = both_scr[pos_ref[qb, block]]
            total = part if total is None else total + part
        return total

    def gsend(h, row):
        return pltpu.make_async_remote_copy(
            src_ref=ysend[h].at[row], dst_ref=yrecv[h].at[row], send_sem=gy_s.at[h, row],
            recv_sem=gy_r.at[h, row], device_id={"kv": partner}, device_id_type=MESH)

    def zcopy(h, row):
        return pltpu.make_async_remote_copy(
            src_ref=zsend[h].at[row], dst_ref=zrecv[h].at[row], send_sem=gz_s.at[h, row],
            recv_sem=gz_r.at[h, row], device_id={"kv": down}, device_id_type=MESH)

    def give(h):
        def other(row, carry):
            def one(k, inner):
                block = (2 * row + 1 - c) * nblk + k
                ysend[h][row, pl.ds(pl.multiple_of(k * BLK, BLK), BLK), :] = block_sum(block).astype(jnp.bfloat16)
                return inner

            lax.fori_loop(0, nblk, one, 0)
            gsend(h, row).start()
            return carry

        lax.fori_loop(0, r + c, other, 0)

        def mine(row, carry):
            def one(k, inner):
                block = (2 * row + c) * nblk + k
                owns[h][row, pl.ds(pl.multiple_of(k * BLK, BLK), BLK), :] = block_sum(block)
                return inner

            lax.fori_loop(0, nblk, one, 0)
            return carry

        lax.fori_loop(0, r + 1, mine, 0)

    def pass_down(h, row):
        gsend(h, row).wait_recv()

        @pl.when(has_up)
        def _():
            zcopy(h, row).wait_recv()
            zsend[h][row] = (
                owns[h][row] + yrecv[h][row].astype(jnp.float32) + zrecv[h][row].astype(jnp.float32)
            ).astype(jnp.bfloat16)

        @pl.when(jnp.logical_not(has_up))
        def _():
            zsend[h][row] = (owns[h][row] + yrecv[h][row].astype(jnp.float32)).astype(jnp.bfloat16)

        zcopy(h, row).start()

    def pass_all(h):
        def step(row, carry):
            pass_down(h, row)
            return carry

        lax.fori_loop(0, r, step, 0)

    def keep(h):
        cols = slice(h * 2 * DH, (h + 1) * 2 * DH)
        kvg_ref[:, cols] = owns[h][r]

        @pl.when(c == 0)
        def _():
            gsend(h, r).wait_recv()
            kvg_ref[:, cols] += yrecv[h][r].astype(jnp.float32)

        @pl.when(has_up)
        def _():
            zcopy(h, r).wait_recv()
            kvg_ref[:, cols] += zrecv[h][r].astype(jnp.float32)

    def rcopy(h, u, s):
        return pltpu.make_async_remote_copy(
            src_ref=rsend[h].at[u, s], dst_ref=rrecv[h].at[u, s], send_sem=r_s.at[h, u, s],
            recv_sem=r_r.at[h, u, s], device_id={"kv": ring_to[u * 2 // SUBS]}, device_id_type=MESH)

    half = width // 2

    def partial_of(h, d, target):
        chunk = inp[target]
        total = None
        for qb in range(nqb):
            part = jnp.dot(qts[h][qb, d * half:(d + 1) * half, :], chunk[qb * QB:(qb + 1) * QB, :],
                           preferred_element_type=jnp.float32)
            total = part if total is None else total + part
        return total

    def ring(h, s, first):
        for d in range(2):
            target = at_pos(pos_me - 1 - s) if d == 0 else at_pos(pos_me + 1 + s)
            part = partial_of(h, d, target)
            for v in range(SUBS // 2):
                u = d * (SUBS // 2) + v
                piece = part[v * sub_w:(v + 1) * sub_w]
                if not first:
                    rcopy(h, u, s - 1).wait_recv()
                    piece = piece + rrecv[h][u, s - 1].astype(jnp.float32)
                rsend[h][u, s] = piece.astype(jnp.bfloat16)
                rcopy(h, u, s).start()

    def ring_end(h):
        for d in range(2):
            part = partial_of(h, d, me)
            got = []
            for v in range(SUBS // 2):
                u = d * (SUBS // 2) + v
                rcopy(h, u, n - 2).wait_recv()
                got.append(part[v * sub_w:(v + 1) * sub_w] + rrecv[h][u, n - 2].astype(jnp.float32))
            wg_ref[:, h * width + d * half:h * width + (d + 1) * half] = jnp.concatenate(got, axis=0).T

    for h in range(kv_heads):
        forward(h, 0)
    for k in range(1, rows_n):
        forward(0, k)
    arrived(0)

    late = kv_heads > 1
    done = 0
    for h in range(kv_heads):
        def loop(qb, carry, h=h):
            attend(h, qb)
            if h + 1 < kv_heads:
                for k in range(1, rows_n):
                    @pl.when(qb == min(k - 1, nqb - 1))
                    def _():
                        forward(h + 1, k)
            return carry

        lax.fori_loop(0, nqb, loop, 0)
        give(h)
        if h == 0:
            for cp in inp_cp:
                cp.wait()
        ring(h, 0, True)
        if h + 1 < kv_heads:
            arrived(h + 1)

    for h in range(kv_heads):
        pass_all(h)

    def ring_loop(s, carry):
        for h in range(kv_heads):
            ring(h, s, False)
        return carry

    lax.fori_loop(1, n - 1, ring_loop, 0)
    for h in range(kv_heads):
        keep(h)
        ring_end(h)

    for h in range(kv_heads):
        for k in range(rows_n):
            @pl.when((r >= k) & has_up)
            def _():
                fetch(h, 2 * (r - k) + c, fz_s, k, up).wait_send()

            @pl.when((r >= k) if k > 0 else (c == 0))
            def _():
                fetch(h, 2 * (r - k) + c, fy_s, k, partner).wait_send()

        def drain_y(row, carry, h=h):
            gsend(h, row).wait_send()
            return carry

        def drain_z(row, carry, h=h):
            zcopy(h, row).wait_send()
            return carry

        lax.fori_loop(0, r + c, drain_y, 0)
        lax.fori_loop(0, r, drain_z, 0)

        def drain_r(s, carry, h=h):
            for u in range(SUBS):
                rcopy(h, u, s).wait_send()
            return carry

        lax.fori_loop(0, n - 1, drain_r, 0)


def shards(queries, keys_values, log_sums, out_grad, inputs, chosen):
    tok = queries.shape[0]
    heads_here = queries.shape[1] // DH
    kv_heads = keys_values.shape[1] // (2 * DH)
    group = heads_here // kv_heads
    nqb, nblk = tok // QB, tok // BLK
    n = lax.axis_size("kv")
    rows_n = n // 2
    lanes = group * QB
    width = group * DH
    sub_w = width // SUBS
    drow = inputs.shape[1] // n
    flat = jnp.arange(nqb * NSEL, dtype=jnp.int32).reshape(nqb, NSEL)
    one_hot = chosen[:, None, :] == jnp.arange(n * nblk, dtype=jnp.int32)[None, :, None]
    zero_at = nqb * NSEL
    pos = zero_at + jnp.sum(jnp.where(one_hot, flat[:, None, :] - zero_at, 0), axis=2)
    start = jnp.maximum(chosen, 0)
    first = jnp.where(chosen >= 0, chosen * BLK, 1 << 30)
    sums = (
        log_sums.reshape(nqb, QB, kv_heads, group).transpose(2, 0, 3, 1).reshape(kv_heads * nqb, 1, lanes)
    )
    vmem = pl.BlockSpec(memory_space=pltpu.VMEM)
    smem = pl.BlockSpec(memory_space=pltpu.SMEM)
    hbm = pl.BlockSpec(memory_space=pl.ANY)
    per_head = lambda shape, dtype: [pltpu.VMEM(shape, dtype)] * kv_heads
    bf, f32 = jnp.bfloat16, jnp.float32
    keys = NSEL * BLK
    dma = pltpu.SemaphoreType.DMA
    scratch = (
        per_head((n * nblk, BLK, 2 * DH), bf)
        + per_head((nqb, width, QB), bf)
        + per_head((rows_n, tok, 2 * DH), f32)
        + per_head((rows_n, tok, 2 * DH), bf)
        + per_head((rows_n, tok, 2 * DH), bf)
        + per_head((rows_n, tok, 2 * DH), bf)
        + per_head((rows_n, tok, 2 * DH), bf)
        + per_head((SUBS, n - 1, sub_w, drow), bf)
        + per_head((SUBS, n - 1, sub_w, drow), bf)
        + [
            pltpu.VMEM((n, tok, drow), bf),
            pltpu.VMEM((2 * DH, 2 * lanes), bf),
            pltpu.VMEM((keys, 2 * DH), bf),
            pltpu.VMEM((keys, lanes), f32),
            pltpu.VMEM((keys, lanes), f32),
            pltpu.VMEM((keys, 2 * lanes), bf),
            pltpu.VMEM((nqb * NSEL + 1, BLK, 2 * DH), f32),
            dma((n,)),
            dma((kv_heads,)),
            dma((kv_heads, rows_n)),
            dma((kv_heads, rows_n)),
            dma((kv_heads, n)),
            dma((kv_heads, rows_n)),
            dma((kv_heads, rows_n)),
            dma((kv_heads, rows_n)),
            dma((kv_heads, rows_n)),
            dma((kv_heads, SUBS, n - 1)),
            dma((kv_heads, SUBS, n - 1)),
        ]
    )
    return pl.pallas_call(
        functools.partial(whole, n, kv_heads, group, tok),
        in_specs=[smem, smem, smem, vmem, vmem, vmem, hbm, hbm],
        out_specs=[vmem, vmem, vmem],
        out_shape=[
            jax.ShapeDtypeStruct((tok, heads_here * DH), bf),
            jax.ShapeDtypeStruct((tok, kv_heads * 2 * DH), f32),
            jax.ShapeDtypeStruct((drow, heads_here * DH), f32),
        ],
        scratch_shapes=scratch,
        compiler_params=pltpu.CompilerParams(
            collective_id=0, has_side_effects=True, vmem_limit_bytes=63 * 1024 * 1024
        ),
    )(start, first, pos.astype(jnp.int32), queries, out_grad, sums, keys_values.reshape(nblk, BLK, -1), inputs)


def solution(mesh):
    in_specs = (
        P("kv", "tp"),
        P("kv", "tp"),
        P("kv", "tp"),
        P("kv", "tp"),
        P("kv", None),
        P("kv", None),
    )
    out_specs = (P("kv", "tp"), P("kv", "tp"), P("kv", "tp"))
    return jax.shard_map(shards, mesh=mesh, in_specs=in_specs, out_specs=out_specs, check_vma=False)
```

```python
import functools

import jax
import jax.numpy as jnp
from jax import lax
from jax.experimental import pallas as pl
from jax.experimental.pallas import tpu as pltpu
from jax.sharding import PartitionSpec as P

DH = 64
BLK = 64
QB = 128
NSEL = 16
CHUNK = 4
SCALE = DH ** (-0.5)
MESH = pl.DeviceIdType.MESH
SUBS = 4
PIECES = 2


def whole(n, kv_heads, group, tok, chosen_ref, list_ref, ls_ref, q_hbm, do_hbm, kv_hbm, inp_hbm,
          dq_hbm, kvg_hbm, wg_hbm, *scratch):
    it = iter(scratch)
    tabs = [next(it) for _ in range(kv_heads)]
    qts = [next(it) for _ in range(kv_heads)]
    owns = [next(it) for _ in range(kv_heads)]
    rows_n = n // 2
    arr = [[next(it) for _ in range(rows_n)] for _ in range(kv_heads)]
    stage = [[next(it) for _ in range(rows_n)] for _ in range(kv_heads)]
    ysend = [next(it) for _ in range(kv_heads)]
    yrecv = [[next(it) for _ in range(rows_n)] for _ in range(kv_heads)]
    zsend = [next(it) for _ in range(kv_heads)]
    zrecv = [next(it) for _ in range(kv_heads)]
    rsend = [next(it) for _ in range(kv_heads)]
    rrecv = [next(it) for _ in range(kv_heads)]
    inp, w1, kv_scr, p_scr, dp_scr, a_scr, both_scr = [next(it) for _ in range(7)]
    q_ref, do_ref, ls_t, dq_ref, kvg_ref, wg_ref, table_v, pos_v, req_v, plist_v, pch_v = [next(it) for _ in range(11)]
    table, pos_ref, req_ref, pch_ref = [next(it) for _ in range(4)]
    (inp_sem, own_sem, in_sem, tab_sem, out_sem, list_sem, loc_sem, fz_s, fy_s, fy_r, f_r, gy_s, gy_r, gz_s, gz_r, r_s, r_r) = [next(it) for _ in range(17)]

    nqb = tok // QB
    nblk = tok // BLK
    cap = nblk // 2
    blocks = n * nblk
    compact = rows_n * nblk
    lanes = group * QB
    width = group * DH
    sub_w = width // SUBS
    me = lax.axis_index("kv")
    r, c = me // 2, me % 2
    partner = 2 * r + 1 - c
    up, down = me + 2, me - 2
    has_up, has_down = r < rows_n - 1, r > 0

    def at_pos(p):
        p = lax.rem(p + 2 * n, n)
        return jnp.where(p < rows_n, 2 * p, 2 * (n - 1 - p) + 1)

    pos_me = jnp.where(c == 0, r, n - 1 - r)
    ring_to = (at_pos(pos_me + 1), at_pos(pos_me - 1))

    barrier = pltpu.get_barrier_semaphore()
    pl.semaphore_signal(barrier, inc=1, device_id={"kv": partner}, device_id_type=MESH)

    @pl.when(has_up)
    def _():
        pl.semaphore_signal(barrier, inc=1, device_id={"kv": up}, device_id_type=MESH)

    @pl.when(has_down)
    def _():
        pl.semaphore_signal(barrier, inc=1, device_id={"kv": down}, device_id_type=MESH)

    own_cp = [
        pltpu.make_async_copy(kv_hbm.at[:, :, h * 2 * DH:(h + 1) * 2 * DH], arr[h][0], own_sem.at[h])
        for h in range(kv_heads)
    ]
    for cp in own_cp:
        cp.start()
    drow = inp_hbm.shape[1] // n
    inp_cp = [
        pltpu.make_async_copy(inp_hbm.at[:, i * drow:(i + 1) * drow], inp.at[i], inp_sem.at[i]) for i in range(n)
    ]
    for cp in inp_cp:
        cp.start()
    in_cp = [
        pltpu.make_async_copy(q_hbm, q_ref, in_sem.at[0]),
        pltpu.make_async_copy(do_hbm, do_ref, in_sem.at[1]),
    ]
    for cp in in_cp:
        cp.start()
    for cp in own_cp:
        cp.wait()
    pl.semaphore_wait(barrier, 1 + has_up.astype(jnp.int32) + has_down.astype(jnp.int32))

    piece_n = nblk // PIECES

    def zfetch(h, k, f):
        src = arr[h][k].at[f * piece_n:(f + 1) * piece_n]
        dst = arr[h][min(k + 1, rows_n - 1)].at[f * piece_n:(f + 1) * piece_n]
        return pltpu.make_async_remote_copy(
            src_ref=src, dst_ref=dst, send_sem=fz_s.at[h, f, k], recv_sem=f_r.at[h, f, min(k + 1, rows_n - 1)],
            device_id={"kv": up}, device_id_type=MESH)

    def yfetch(h, k):
        return pltpu.make_async_remote_copy(
            src_ref=stage[h][k], dst_ref=tabs[h].at[pl.ds(compact + (r - k) * cap, cap)], send_sem=fy_s.at[h, k],
            recv_sem=fy_r.at[h, k], device_id={"kv": partner}, device_id_type=MESH)

    def local(h, k):
        return pltpu.make_async_copy(arr[h][k], tabs[h].at[pl.ds((r - k) * nblk, nblk)], loc_sem.at[h, k])

    def forward(h, k, f):
        @pl.when(r >= k)
        def _():
            if k > 0:
                zfetch(h, k - 1, f).wait_recv()
            if k < rows_n - 1:
                @pl.when(has_up)
                def _():
                    zfetch(h, k, f).start()

    def across(h, k):
        @pl.when(r >= k)
        def _():
            local(h, k).start()

            @pl.when((c == 0) if k == 0 else (c >= 0))
            def _():
                owner = 2 * (r - k) + c
                for i in range(cap):
                    stage[h][k][i] = arr[h][k][req_ref[n + owner, i]]
                yfetch(h, k).start()

    def arrived(h):
        for k in range(rows_n):
            @pl.when((r >= k) if k > 0 else (c == 1))
            def _():
                yfetch(h, k).wait_recv()

            @pl.when(r >= k)
            def _():
                local(h, k).wait()

    def attend(h, qb):
        tab = tabs[h]
        qrow = pl.ds(pl.multiple_of(qb * QB, QB), QB)
        cols = slice(h * width, (h + 1) * width)
        q_t = (q_ref[qrow, cols].astype(jnp.float32) * SCALE).T.astype(jnp.bfloat16)
        do_t = do_ref[qrow, cols].astype(jnp.float32).T.astype(jnp.bfloat16)
        for g in range(group):
            w1[:DH, g * QB:(g + 1) * QB] = q_t[g * DH:(g + 1) * DH]
            w1[DH:, lanes + g * QB:lanes + (g + 1) * QB] = do_t[g * DH:(g + 1) * DH]
        for j in range(NSEL):
            kv_scr[j * BLK:(j + 1) * BLK, :] = tab[pos_ref[nqb, table[qb, j]]]
        rows = CHUNK * BLK
        lane = lax.broadcasted_iota(jnp.int32, (1, lanes), 1)
        qpos = (me * nqb + qb) * QB + lax.rem(lane, QB)
        within = lax.broadcasted_iota(jnp.int32, (BLK, lanes), 0)
        sums = jnp.concatenate([ls_t[qb, h * group + g:h * group + g + 1, :] for g in range(group)], axis=1)
        delta = jnp.zeros((1, lanes), jnp.float32)
        for ch in range(NSEL // CHUNK):
            kv = kv_scr[ch * rows:(ch + 1) * rows, :]
            scores = jnp.dot(kv, w1[:, :lanes], preferred_element_type=jnp.float32)
            grads = jnp.dot(kv, w1[:, lanes:], preferred_element_type=jnp.float32)
            for i in range(CHUNK):
                last = qpos - table[qb, NSEL + ch * CHUNK + i]
                here = slice(i * BLK, (i + 1) * BLK)
                there = slice(ch * rows + i * BLK, ch * rows + (i + 1) * BLK)
                prob = jnp.where(within <= last, jnp.exp(scores[here] - sums), jnp.float32(0.0))
                rounded = prob.astype(jnp.bfloat16)
                delta += jnp.sum(rounded.astype(jnp.float32) * grads[here], axis=0, keepdims=True)
                p_scr[there, :] = prob
                dp_scr[there, :] = grads[here]
                a_scr[there, lanes:] = rounded
        for ch in range(NSEL // CHUNK):
            there = slice(ch * rows, (ch + 1) * rows)
            a_scr[there, :lanes] = (p_scr[there, :] * (dp_scr[there, :] - delta)).astype(jnp.bfloat16)
            both_scr[pl.ds(qb * NSEL + ch * CHUNK, CHUNK)] = lax.dot_general(
                a_scr[there, :], w1[...], (((1,), (1,)), ((), ())), preferred_element_type=jnp.float32
            ).reshape(CHUNK, BLK, 2 * DH)
        dq_t = jnp.dot(kv_scr[...].T, a_scr[:, :lanes], preferred_element_type=jnp.float32)[:DH] * SCALE
        stacked = jnp.concatenate([dq_t[:, g * QB:(g + 1) * QB] for g in range(group)], axis=0)
        qts[h][qb] = stacked.astype(jnp.bfloat16)
        dq_ref[qrow, cols] = stacked.T.astype(jnp.bfloat16)

    def block_sum(block):
        total = None
        for qb in range(nqb):
            part = both_scr[pos_ref[qb, block]]
            total = part if total is None else total + part
        return total

    def gsend(h, row):
        return pltpu.make_async_remote_copy(
            src_ref=ysend[h].at[row], dst_ref=yrecv[h][row].at[:cap], send_sem=gy_s.at[h, row],
            recv_sem=gy_r.at[h, row], device_id={"kv": partner}, device_id_type=MESH)

    def zcopy(h, row):
        return pltpu.make_async_remote_copy(
            src_ref=zsend[h].at[row], dst_ref=zrecv[h].at[row], send_sem=gz_s.at[h, row],
            recv_sem=gz_r.at[h, row], device_id={"kv": down}, device_id_type=MESH)

    def give(h):
        for row in range(rows_n):
            @pl.when(row < r + c)
            def _():
                def one(k, inner):
                    owner = 2 * row + 1 - c
                    ysend[h][row, k] = block_sum(owner * nblk + req_ref[owner, k]).astype(jnp.bfloat16)
                    return inner

                lax.fori_loop(0, cap, one, 0)
                gsend(h, row).start()

        def mine(i, carry):
            row, k = i // nblk, i % nblk
            owns[h][row, k] = block_sum((2 * row + c) * nblk + k)
            return carry

        lax.fori_loop(0, (r + 1) * nblk, mine, 0)

    def pass_down(h, row):
        gsend(h, row).wait_recv()

        @pl.when(has_up)
        def _():
            zcopy(h, row).wait_recv()

        def one(k, carry):
            total = owns[h][row, k] + yrecv[h][row][pos_ref[nqb + 1, (2 * row + c) * nblk + k]].astype(jnp.float32)

            @pl.when(has_up)
            def _():
                zsend[h][row, k] = (total + zrecv[h][row, k].astype(jnp.float32)).astype(jnp.bfloat16)

            @pl.when(jnp.logical_not(has_up))
            def _():
                zsend[h][row, k] = total.astype(jnp.bfloat16)

            return carry

        lax.fori_loop(0, nblk, one, 0)
        zcopy(h, row).start()

    def keep(h):
        cols = slice(h * 2 * DH, (h + 1) * 2 * DH)

        @pl.when(has_up)
        def _():
            zcopy(h, r).wait_recv()
            kvg_ref[:, cols] = (owns[h][r] + zrecv[h][r].astype(jnp.float32)).reshape(tok, 2 * DH)

        @pl.when(jnp.logical_not(has_up))
        def _():
            kvg_ref[:, cols] = owns[h][r].reshape(tok, 2 * DH)

        for row in range(rows_n):
            @pl.when((c == 0) & (r == row))
            def _():
                gsend(h, row).wait_recv()
                for k in range(nblk):
                    kvg_ref[k * BLK:(k + 1) * BLK, cols] += (
                        yrecv[h][row][pos_ref[nqb + 1, (2 * row + c) * nblk + k]].astype(jnp.float32))

    def rcopy(h, u, s):
        return pltpu.make_async_remote_copy(
            src_ref=rsend[h].at[u, s], dst_ref=rrecv[h].at[u, s], send_sem=r_s.at[h, u, s],
            recv_sem=r_r.at[h, u, s], device_id={"kv": ring_to[u * 2 // SUBS]}, device_id_type=MESH)

    half = width // 2

    def partial_of(h, d, target):
        chunk = inp[target]
        total = None
        for qb in range(nqb):
            part = jnp.dot(qts[h][qb, d * half:(d + 1) * half, :], chunk[qb * QB:(qb + 1) * QB, :],
                           preferred_element_type=jnp.float32)
            total = part if total is None else total + part
        return total

    def ring(h, s, first):
        for d in range(2):
            target = at_pos(pos_me - 1 - s) if d == 0 else at_pos(pos_me + 1 + s)
            part = partial_of(h, d, target)
            for v in range(SUBS // 2):
                u = d * (SUBS // 2) + v
                piece = part[v * sub_w:(v + 1) * sub_w]
                if not first:
                    rcopy(h, u, s - 1).wait_recv()
                    piece = piece + rrecv[h][u, s - 1].astype(jnp.float32)
                rsend[h][u, s] = piece.astype(jnp.bfloat16)
                rcopy(h, u, s).start()

    def ring_end():
        parts = [[partial_of(h, d, me) for d in range(2)] for h in range(kv_heads)]
        for h in range(kv_heads):
            for d in range(2):
                got = []
                for v in range(SUBS // 2):
                    u = d * (SUBS // 2) + v
                    rcopy(h, u, n - 2).wait_recv()
                    got.append(parts[h][d][v * sub_w:(v + 1) * sub_w] + rrecv[h][u, n - 2].astype(jnp.float32))
                wg_ref[:, h * width + d * half:h * width + (d + 1) * half] = jnp.concatenate(got, axis=0).T

    def pass_slot(h, slot):
        for row in range(rows_n - 1):
            @pl.when((slot - (rows_n - 1 - r) == row) & (row < r))
            def _():
                with jax.named_scope(f"pass{h}"):
                    pass_down(h, row)

    list_cp = pltpu.make_async_remote_copy(
        src_ref=list_ref, dst_ref=plist_v, send_sem=list_sem.at[0], recv_sem=list_sem.at[1],
        device_id={"kv": partner}, device_id_type=MESH)
    list_cp.start()

    def ranks(ref, ids, within):
        need = ids == ref[0, 0]
        for qb in range(nqb):
            for j in range(NSEL):
                need = need | (ids == ref[qb, j])
        need = need.astype(jnp.int32)
        rank = jnp.zeros_like(need)
        for d in range(1, nblk):
            rank = rank + jnp.where(within >= d, pltpu.roll(need, d, 1), 0)
        return need, rank

    def wanted(need, rank, within, owner):
        out = jnp.zeros((n, 128), jnp.int32)
        lane = lax.broadcasted_iota(jnp.int32, (n, 128), 1)
        here = owner == lax.broadcasted_iota(jnp.int32, (n, pos_v.shape[1]), 0)
        for k in range(cap):
            hit = here & (need == 1) & (rank == k)
            out = jnp.where(lane == k, jnp.sum(jnp.where(hit, within, 0), axis=1, keepdims=True), out)
        return out

    with jax.named_scope("fetch_first"):
        for h in range(kv_heads):
            for f in range(PIECES):
                forward(h, 0, f)
        ids = lax.broadcasted_iota(jnp.int32, (1, pos_v.shape[1]), 1)
        owner = jnp.zeros_like(ids)
        for o in range(1, n):
            owner = owner + (ids >= o * nblk).astype(jnp.int32)
        within = ids - owner * nblk
        line = owner // 2
        own_col = owner - 2 * line == c
        need, rank = ranks(chosen_ref, ids, within)
        pos_v[nqb:nqb + 1, :] = jnp.where(own_col, line * nblk + within, compact + line * cap + rank)
        req_v[:n] = wanted(need, rank, within, owner)
        listed = list_ref[...]
        table_v[:nqb, :NSEL] = jnp.maximum(listed, 0)
        table_v[:nqb, NSEL:2 * NSEL] = jnp.where(listed >= 0, listed * BLK, 1 << 30)
        for qb in range(nqb):
            at = jnp.full(ids.shape, nqb * NSEL, jnp.int32)
            for j in range(NSEL):
                at = jnp.where(ids == chosen_ref[qb, j], qb * NSEL + j, at)
            pos_v[qb:qb + 1, :] = at
        list_cp.wait_recv()
        pch_v[:nqb, :NSEL] = plist_v[...]
        cp = pltpu.make_async_copy(pch_v, pch_ref, tab_sem.at[0])
        cp.start()
        cp.wait()
        need, rank = ranks(pch_ref, ids, within)
        pos_v[nqb + 1:nqb + 2, :] = jnp.where(need == 1, rank, cap)
        req_v[n:] = wanted(need, rank, within, owner)
        tab_cp = [
            pltpu.make_async_copy(table_v, table, tab_sem.at[0]),
            pltpu.make_async_copy(pos_v, pos_ref, tab_sem.at[1]),
            pltpu.make_async_copy(req_v, req_ref, tab_sem.at[2]),
        ]
        for cp in tab_cp:
            cp.start()
        for cp in tab_cp:
            cp.wait()
        for h in range(kv_heads):
            across(h, 0)
        for k in range(1, rows_n):
            for f in range(PIECES):
                forward(0, k, f)
            across(0, k)
            if k == 1:
                w1[...] = jnp.zeros_like(w1)
                both_scr[nqb * NSEL] = jnp.zeros((BLK, 2 * DH), jnp.float32)
                for h in range(kv_heads):
                    for row in range(rows_n):
                        yrecv[h][row][cap] = jnp.zeros((BLK, 2 * DH), jnp.bfloat16)
                for qb in range(nqb):
                    ls_t[qb] = ls_ref[:, qb * QB:(qb + 1) * QB]
        arrived(0)
        for cp in in_cp:
            cp.wait()

    early = [nqb // 2 if h + 1 < kv_heads else 0 for h in range(kv_heads)]
    pieces = [(k, f) for k in range(1, rows_n) for f in range(PIECES)]
    dq_cp = []
    for h in range(kv_heads):
        def loop(qb, carry, h=h):
            with jax.named_scope(f"attend{h}"):
                attend(h, qb)
            if h + 1 < kv_heads:
                for i, (k, f) in enumerate(pieces):
                    @pl.when(qb == i * nqb // len(pieces))
                    def _():
                        with jax.named_scope("forward_next"):
                            forward(h + 1, k, f)
                            if f == PIECES - 1:
                                across(h + 1, k)
            if h > 0:
                for k in range(early[h - 1]):
                    @pl.when(qb == 2 * k + 1)
                    def _():
                        with jax.named_scope(f"ring{h - 1}"):
                            ring(h - 1, k + 1, False)
                        pass_slot(h - 1, k)
            return carry

        lax.fori_loop(0, nqb, loop, 0)
        dq_cp.append(pltpu.make_async_copy(
            dq_ref.at[:, h * width:(h + 1) * width], dq_hbm.at[:, h * width:(h + 1) * width], out_sem.at[h]))
        dq_cp[h].start()
        if h == 0:
            for cp in inp_cp:
                cp.wait()
        with jax.named_scope(f"ring_first{h}"):
            ring(h, 0, True)
        with jax.named_scope(f"give{h}"):
            give(h)
        if h + 1 < kv_heads:
            with jax.named_scope("arrive_next"):
                arrived(h + 1)

    def ring_loop(s, carry):
        for h in range(kv_heads):
            @pl.when(s + early[h] <= n - 2)
            def _():
                with jax.named_scope(f"ring{h}"):
                    ring(h, s + early[h], False)
            pass_slot(h, s - 1 + early[h] if early[h] else s - 2)
        return carry

    lax.fori_loop(1, n - 1, ring_loop, 0)
    for h in range(kv_heads):
        with jax.named_scope(f"keep{h}"):
            keep(h)
    kvg_cp = pltpu.make_async_copy(kvg_ref, kvg_hbm, out_sem.at[kv_heads])
    kvg_cp.start()
    with jax.named_scope("ring_end"):
        ring_end()
    wg_cp = pltpu.make_async_copy(wg_ref, wg_hbm, out_sem.at[kv_heads + 1])
    wg_cp.start()

    list_cp.wait_send()
    for h in range(kv_heads):
        for k in range(rows_n):
            if k < rows_n - 1:
                @pl.when((r >= k) & has_up)
                def _():
                    for f in range(PIECES):
                        zfetch(h, k, f).wait_send()

            @pl.when((r >= k) if k > 0 else (c == 0))
            def _():
                yfetch(h, k).wait_send()

        for row in range(rows_n):
            @pl.when(row < r + c)
            def _():
                gsend(h, row).wait_send()

            @pl.when(row < r)
            def _():
                zcopy(h, row).wait_send()

        def drain_r(s, carry, h=h):
            for u in range(SUBS):
                rcopy(h, u, s).wait_send()
            return carry

        lax.fori_loop(0, n - 1, drain_r, 0)
    for cp in dq_cp + [kvg_cp, wg_cp]:
        cp.wait()


def hand_on(*refs):
    srcs, dsts, bufs, sems = refs[:3], refs[3:6], refs[6:9], refs[9]
    pieces = []
    for i in range(3):
        step = srcs[i].shape[0] // 2
        for k in range(2):
            rows = slice(k * step, (k + 1) * step)
            pieces.append((
                pltpu.make_async_copy(srcs[i].at[rows], bufs[i].at[rows], sems.at[0, i, k]),
                pltpu.make_async_copy(bufs[i].at[rows], dsts[i].at[rows], sems.at[1, i, k])))
    for load, _ in pieces:
        load.start()
    for load, store in pieces:
        load.wait()
        store.start()
    for _, store in pieces:
        store.wait()


def shards(queries, keys_values, log_sums, out_grad, inputs, chosen):
    tok = queries.shape[0]
    heads_here = queries.shape[1] // DH
    kv_heads = keys_values.shape[1] // (2 * DH)
    group = heads_here // kv_heads
    nqb, nblk = tok // QB, tok // BLK
    n = lax.axis_size("kv")
    rows_n = n // 2
    row_width = keys_values.shape[1]
    cap = nblk // 2
    pos_w = pl.cdiv(n * nblk, 128) * 128
    lanes = group * QB
    width = group * DH
    sub_w = width // SUBS
    drow = inputs.shape[1] // n
    vmem = pl.BlockSpec(memory_space=pltpu.VMEM)
    smem = pl.BlockSpec(memory_space=pltpu.SMEM)
    hbm = pl.BlockSpec(memory_space=pl.ANY)
    per_head = lambda shape, dtype: [pltpu.VMEM(shape, dtype)] * kv_heads
    bf, f32 = jnp.bfloat16, jnp.float32
    keys = NSEL * BLK
    dma = pltpu.SemaphoreType.DMA
    scratch = (
        per_head((rows_n * (nblk + cap), BLK, 2 * DH), bf)
        + per_head((nqb, width, QB), bf)
        + per_head((rows_n, nblk, BLK, 2 * DH), f32)
        + per_head((nblk, BLK, 2 * DH), bf) * rows_n
        + per_head((cap, BLK, 2 * DH), bf) * rows_n
        + per_head((rows_n, cap, BLK, 2 * DH), bf)
        + per_head((cap + 1, BLK, 2 * DH), bf) * rows_n
        + per_head((rows_n, nblk, BLK, 2 * DH), bf)
        + per_head((rows_n, nblk, BLK, 2 * DH), bf)
        + per_head((SUBS, n - 1, sub_w, drow), bf)
        + per_head((SUBS, n - 1, sub_w, drow), bf)
        + [
            pltpu.VMEM((n, tok, drow), bf),
            pltpu.VMEM((2 * DH, 2 * lanes), bf),
            pltpu.VMEM((keys, 2 * DH), bf),
            pltpu.VMEM((keys, lanes), f32),
            pltpu.VMEM((keys, lanes), f32),
            pltpu.VMEM((keys, 2 * lanes), bf),
            pltpu.VMEM((nqb * NSEL + 1, BLK, 2 * DH), f32),
            pltpu.VMEM((tok, heads_here * DH), bf),
            pltpu.VMEM((tok, heads_here * DH), bf),
            pltpu.VMEM((nqb, heads_here, QB), f32),
            pltpu.VMEM((tok, heads_here * DH), bf),
            pltpu.VMEM((tok, row_width), f32),
            pltpu.VMEM((drow, heads_here * DH), f32),
            pltpu.VMEM((8, 128), jnp.int32),
            pltpu.VMEM((8, pos_w), jnp.int32),
            pltpu.VMEM((2 * n, 128), jnp.int32),
            pltpu.VMEM((nqb, NSEL), jnp.int32),
            pltpu.VMEM((8, 128), jnp.int32),
            pltpu.SMEM((8, 128), jnp.int32),
            pltpu.SMEM((8, pos_w), jnp.int32),
            pltpu.SMEM((2 * n, 128), jnp.int32),
            pltpu.SMEM((8, 128), jnp.int32),
            dma((n,)),
            dma((kv_heads,)),
            dma((2,)),
            dma((3,)),
            dma((kv_heads + 2,)),
            dma((2,)),
            dma((kv_heads, rows_n)),
            dma((kv_heads, PIECES, rows_n)),
            dma((kv_heads, rows_n)),
            dma((kv_heads, rows_n)),
            dma((kv_heads, PIECES, rows_n)),
            dma((kv_heads, rows_n)),
            dma((kv_heads, rows_n)),
            dma((kv_heads, rows_n)),
            dma((kv_heads, rows_n)),
            dma((kv_heads, SUBS, n - 1)),
            dma((kv_heads, SUBS, n - 1)),
        ]
    )
    shapes = [
        jax.ShapeDtypeStruct((tok, heads_here * DH), bf),
        jax.ShapeDtypeStruct((tok, row_width), f32),
        jax.ShapeDtypeStruct((drow, heads_here * DH), f32),
    ]
    raw = pl.pallas_call(
        functools.partial(whole, n, kv_heads, group, tok),
        in_specs=[smem, vmem, vmem, hbm, hbm, hbm, hbm],
        out_specs=[hbm, hbm, hbm],
        out_shape=shapes,
        scratch_shapes=scratch,
        compiler_params=pltpu.CompilerParams(
            collective_id=0, has_side_effects=True, vmem_limit_bytes=63 * 1024 * 1024
        ),
    )(chosen, chosen, log_sums.T, queries, out_grad, keys_values.reshape(nblk, BLK, -1), inputs)
    return tuple(pl.pallas_call(
        hand_on,
        in_specs=[hbm] * 3,
        out_specs=[hbm] * 3,
        out_shape=shapes,
        scratch_shapes=[pltpu.VMEM(x.shape, x.dtype) for x in shapes] + [dma((2, 3, 2))],
    )(*raw))


def solution(mesh):
    in_specs = (
        P("kv", "tp"),
        P("kv", "tp"),
        P("kv", "tp"),
        P("kv", "tp"),
        P("kv", None),
        P("kv", None),
    )
    out_specs = (P("kv", "tp"), P("kv", "tp"), P("kv", "tp"))
    return jax.shard_map(shards, mesh=mesh, in_specs=in_specs, out_specs=out_specs, check_vma=False)
```

```python
import functools

import jax
import jax.numpy as jnp
from jax import lax
from jax.experimental import pallas as pl
from jax.experimental.pallas import tpu as pltpu
from jax.sharding import PartitionSpec as P

DH = 64
BLK = 64
QB = 128
NSEL = 16
CHUNK = 4
SCALE = DH ** (-0.5)
MESH = pl.DeviceIdType.MESH
SUBS = 4
PIECES = 2
OFFS = (1, 3)


def whole(n, kv_heads, group, tok, chosen_hbm, ls_hbm, q_hbm, do_hbm, kv_hbm, inp_hbm,
          dq_hbm, kvg_hbm, wg_hbm, *scratch):
    it = iter(scratch)
    tabs = [next(it) for _ in range(kv_heads)]
    qts = [next(it) for _ in range(kv_heads)]
    owns = [next(it) for _ in range(kv_heads)]
    rows_n = n // 2
    arr = [[next(it) for _ in range(rows_n)] for _ in range(kv_heads)]
    stage = [[next(it) for _ in range(rows_n)] for _ in range(kv_heads)]
    ysend = [next(it) for _ in range(kv_heads)]
    yrecv = [[next(it) for _ in range(rows_n)] for _ in range(kv_heads)]
    zsend = [next(it) for _ in range(kv_heads)]
    zrecv = [next(it) for _ in range(kv_heads)]
    rsend = [next(it) for _ in range(kv_heads)]
    rrecv = [next(it) for _ in range(kv_heads)]
    inp, w1, kv_scr, p_scr, dp_scr, a_scr, both_scr = [next(it) for _ in range(7)]
    q_ref, do_ref, ls_t, dq_ref, kvg_ref, wg_ref, table_v, pos_v, req_v, plist_v, pch_v = [next(it) for _ in range(11)]
    table, pos_ref, req_ref, pch_ref, chosen_ref, list_ref, ls_ref = [next(it) for _ in range(7)]
    (inp_sem, own_sem, in_sem, tab_sem, out_sem, list_sem, loc_sem, fz_s, fy_s, fy_r, f_r, gy_s, gy_r, gz_s, gz_r, r_s, r_r) = [next(it) for _ in range(17)]

    nqb = tok // QB
    nblk = tok // BLK
    cap = nblk // 2
    blocks = n * nblk
    compact = rows_n * nblk
    lanes = group * QB
    width = group * DH
    sub_w = width // SUBS
    me = lax.axis_index("kv")
    r, c = me // 2, me % 2
    partner = 2 * r + 1 - c
    up, down = me + 2, me - 2
    has_up, has_down = r < rows_n - 1, r > 0

    def at_pos(p):
        p = lax.rem(p + 2 * n, n)
        return jnp.where(p < rows_n, 2 * p, 2 * (n - 1 - p) + 1)

    pos_me = jnp.where(c == 0, r, n - 1 - r)
    ring_to = (at_pos(pos_me + 1), at_pos(pos_me - 1))

    own_cp = [
        pltpu.make_async_copy(kv_hbm.at[:, :, h * 2 * DH:(h + 1) * 2 * DH], arr[h][0], own_sem.at[h])
        for h in range(kv_heads)
    ]
    small_cp = [
        pltpu.make_async_copy(chosen_hbm, list_ref, in_sem.at[2]),
        pltpu.make_async_copy(chosen_hbm, chosen_ref, in_sem.at[3]),
        pltpu.make_async_copy(ls_hbm, ls_ref, in_sem.at[4]),
    ]
    for cp in own_cp[:1] + small_cp + own_cp[1:]:
        cp.start()
    barrier = pltpu.get_barrier_semaphore()
    pl.semaphore_signal(barrier, inc=1, device_id={"kv": partner}, device_id_type=MESH)

    @pl.when(has_up)
    def _():
        pl.semaphore_signal(barrier, inc=1, device_id={"kv": up}, device_id_type=MESH)

    @pl.when(has_down)
    def _():
        pl.semaphore_signal(barrier, inc=1, device_id={"kv": down}, device_id_type=MESH)

    drow = inp_hbm.shape[1] // n
    inp_cp = [
        pltpu.make_async_copy(inp_hbm.at[:, i * drow:(i + 1) * drow], inp.at[i], inp_sem.at[i]) for i in range(n)
    ]
    in_cp = [
        pltpu.make_async_copy(q_hbm, q_ref, in_sem.at[0]),
        pltpu.make_async_copy(do_hbm, do_ref, in_sem.at[1]),
    ]
    for cp in in_cp:
        cp.start()
    for cp in inp_cp:
        cp.start()
    own_cp[0].wait()
    pl.semaphore_wait(barrier, 1 + has_up.astype(jnp.int32) + has_down.astype(jnp.int32))

    piece_n = nblk // PIECES

    def zfetch(h, k, f):
        src = arr[h][k].at[f * piece_n:(f + 1) * piece_n]
        dst = arr[h][min(k + 1, rows_n - 1)].at[f * piece_n:(f + 1) * piece_n]
        return pltpu.make_async_remote_copy(
            src_ref=src, dst_ref=dst, send_sem=fz_s.at[h, f, k], recv_sem=f_r.at[h, f, min(k + 1, rows_n - 1)],
            device_id={"kv": up}, device_id_type=MESH)

    def yfetch(h, k):
        return pltpu.make_async_remote_copy(
            src_ref=stage[h][k], dst_ref=tabs[h].at[pl.ds(compact + (r - k) * cap, cap)], send_sem=fy_s.at[h, k],
            recv_sem=fy_r.at[h, k], device_id={"kv": partner}, device_id_type=MESH)

    def local(h, k):
        return pltpu.make_async_copy(arr[h][k], tabs[h].at[pl.ds((r - k) * nblk, nblk)], loc_sem.at[h, k])

    def forward(h, k, f):
        @pl.when(r >= k)
        def _():
            if k > 0:
                zfetch(h, k - 1, f).wait_recv()
            if k < rows_n - 1:
                @pl.when(has_up)
                def _():
                    zfetch(h, k, f).start()

    def across(h, k):
        @pl.when(r >= k)
        def _():
            local(h, k).start()

            @pl.when((c == 0) if k == 0 else (c >= 0))
            def _():
                owner = 2 * (r - k) + c
                for i in range(cap):
                    stage[h][k][i] = arr[h][k][req_ref[n + owner, i]]
                yfetch(h, k).start()

    def arrived(h):
        for k in range(rows_n):
            @pl.when((r >= k) if k > 0 else (c == 1))
            def _():
                yfetch(h, k).wait_recv()

            @pl.when(r >= k)
            def _():
                local(h, k).wait()

    def attend(h, qb):
        tab = tabs[h]
        qrow = pl.ds(pl.multiple_of(qb * QB, QB), QB)
        cols = slice(h * width, (h + 1) * width)
        q_t = (q_ref[qrow, cols].astype(jnp.float32) * SCALE).T.astype(jnp.bfloat16)
        do_t = do_ref[qrow, cols].astype(jnp.float32).T.astype(jnp.bfloat16)
        for g in range(group):
            w1[:DH, g * QB:(g + 1) * QB] = q_t[g * DH:(g + 1) * DH]
            w1[DH:, lanes + g * QB:lanes + (g + 1) * QB] = do_t[g * DH:(g + 1) * DH]
        for j in range(NSEL):
            kv_scr[j * BLK:(j + 1) * BLK, :] = tab[pos_ref[nqb, table[qb, j]]]
        rows = CHUNK * BLK
        lane = lax.broadcasted_iota(jnp.int32, (1, lanes), 1)
        qpos = (me * nqb + qb) * QB + lax.rem(lane, QB)
        within = lax.broadcasted_iota(jnp.int32, (BLK, lanes), 0)
        sums = jnp.concatenate([ls_t[qb, h * group + g:h * group + g + 1, :] for g in range(group)], axis=1)
        delta = jnp.zeros((1, lanes), jnp.float32)
        for ch in range(NSEL // CHUNK):
            kv = kv_scr[ch * rows:(ch + 1) * rows, :]
            scores = jnp.dot(kv, w1[:, :lanes], preferred_element_type=jnp.float32)
            grads = jnp.dot(kv, w1[:, lanes:], preferred_element_type=jnp.float32)
            for i in range(CHUNK):
                last = qpos - table[qb, NSEL + ch * CHUNK + i]
                here = slice(i * BLK, (i + 1) * BLK)
                there = slice(ch * rows + i * BLK, ch * rows + (i + 1) * BLK)
                prob = jnp.where(within <= last, jnp.exp(scores[here] - sums), jnp.float32(0.0))
                rounded = prob.astype(jnp.bfloat16)
                delta += jnp.sum(rounded.astype(jnp.float32) * grads[here], axis=0, keepdims=True)
                p_scr[there, :] = prob
                dp_scr[there, :] = grads[here]
                a_scr[there, lanes:] = rounded
        for ch in range(NSEL // CHUNK):
            there = slice(ch * rows, (ch + 1) * rows)
            a_scr[there, :lanes] = (p_scr[there, :] * (dp_scr[there, :] - delta)).astype(jnp.bfloat16)
            both_scr[pl.ds(qb * NSEL + ch * CHUNK, CHUNK)] = lax.dot_general(
                a_scr[there, :], w1[...], (((1,), (1,)), ((), ())), preferred_element_type=jnp.float32
            ).reshape(CHUNK, BLK, 2 * DH)
        dq_t = jnp.dot(kv_scr[...].T, a_scr[:, :lanes], preferred_element_type=jnp.float32)[:DH] * SCALE
        stacked = jnp.concatenate([dq_t[:, g * QB:(g + 1) * QB] for g in range(group)], axis=0)
        qts[h][qb] = stacked.astype(jnp.bfloat16)
        dq_ref[qrow, cols] = stacked.T.astype(jnp.bfloat16)

    def block_sum(block):
        total = None
        for qb in range(nqb):
            part = both_scr[pos_ref[qb, block]]
            total = part if total is None else total + part
        return total

    def gsend(h, row):
        return pltpu.make_async_remote_copy(
            src_ref=ysend[h].at[row], dst_ref=yrecv[h][row].at[:cap], send_sem=gy_s.at[h, row],
            recv_sem=gy_r.at[h, row], device_id={"kv": partner}, device_id_type=MESH)

    def zcopy(h, row):
        return pltpu.make_async_remote_copy(
            src_ref=zsend[h].at[row], dst_ref=zrecv[h].at[row], send_sem=gz_s.at[h, row],
            recv_sem=gz_r.at[h, row], device_id={"kv": down}, device_id_type=MESH)

    def give(h):
        for row in range(rows_n):
            @pl.when(row < r + c)
            def _():
                def one(k, inner):
                    owner = 2 * row + 1 - c
                    ysend[h][row, k] = block_sum(owner * nblk + req_ref[owner, k]).astype(jnp.bfloat16)
                    return inner

                lax.fori_loop(0, cap, one, 0)
                gsend(h, row).start()

        def mine(i, carry):
            row, k = i // nblk, i % nblk
            owns[h][row, k] = block_sum((2 * row + c) * nblk + k)
            return carry

        lax.fori_loop(0, (r + 1) * nblk, mine, 0)

    def pass_down(h, row):
        gsend(h, row).wait_recv()

        @pl.when(has_up)
        def _():
            zcopy(h, row).wait_recv()

        def one(k, carry):
            total = owns[h][row, k] + yrecv[h][row][pos_ref[nqb + 1, (2 * row + c) * nblk + k]].astype(jnp.float32)

            @pl.when(has_up)
            def _():
                zsend[h][row, k] = (total + zrecv[h][row, k].astype(jnp.float32)).astype(jnp.bfloat16)

            @pl.when(jnp.logical_not(has_up))
            def _():
                zsend[h][row, k] = total.astype(jnp.bfloat16)

            return carry

        lax.fori_loop(0, nblk, one, 0)
        zcopy(h, row).start()

    def keep(h):
        cols = slice(h * 2 * DH, (h + 1) * 2 * DH)

        @pl.when(has_up)
        def _():
            zcopy(h, r).wait_recv()
            kvg_ref[:, cols] = (owns[h][r] + zrecv[h][r].astype(jnp.float32)).reshape(tok, 2 * DH)

        @pl.when(jnp.logical_not(has_up))
        def _():
            kvg_ref[:, cols] = owns[h][r].reshape(tok, 2 * DH)

        for row in range(rows_n):
            @pl.when((c == 0) & (r == row))
            def _():
                gsend(h, row).wait_recv()
                for k in range(nblk):
                    kvg_ref[k * BLK:(k + 1) * BLK, cols] += (
                        yrecv[h][row][pos_ref[nqb + 1, (2 * row + c) * nblk + k]].astype(jnp.float32))

        kvg_cp[h].start()

    def rcopy(h, u, s):
        return pltpu.make_async_remote_copy(
            src_ref=rsend[h].at[u, s], dst_ref=rrecv[h].at[u, s], send_sem=r_s.at[h, u, s],
            recv_sem=r_r.at[h, u, s], device_id={"kv": ring_to[u * 2 // SUBS]}, device_id_type=MESH)

    half = width // 2

    def partial_of(h, d, target):
        chunk = inp[target]
        total = None
        for qb in range(nqb):
            part = jnp.dot(qts[h][qb, d * half:(d + 1) * half, :], chunk[qb * QB:(qb + 1) * QB, :],
                           preferred_element_type=jnp.float32)
            total = part if total is None else total + part
        return total

    def ring(h, s, first):
        for d in range(2):
            target = at_pos(pos_me - 1 - s) if d == 0 else at_pos(pos_me + 1 + s)
            part = partial_of(h, d, target)
            for v in range(SUBS // 2):
                u = d * (SUBS // 2) + v
                piece = part[v * sub_w:(v + 1) * sub_w]
                if not first:
                    rcopy(h, u, s - 1).wait_recv()
                    piece = piece + rrecv[h][u, s - 1].astype(jnp.float32)
                rsend[h][u, s] = piece.astype(jnp.bfloat16)
                rcopy(h, u, s).start()

    def ring_end(h):
        parts = [partial_of(h, d, me) for d in range(2)]
        for d in range(2):
            got = []
            for v in range(SUBS // 2):
                u = d * (SUBS // 2) + v
                rcopy(h, u, n - 2).wait_recv()
                got.append(parts[d][v * sub_w:(v + 1) * sub_w] + rrecv[h][u, n - 2].astype(jnp.float32))
            wg_ref[:, h * width + d * half:h * width + (d + 1) * half] = jnp.concatenate(got, axis=0).T
        wg_cp[h].start()

    def pass_slot(h, slot):
        for row in range(rows_n - 1):
            @pl.when((slot - (rows_n - 1 - r) == row) & (row < r))
            def _():
                with jax.named_scope(f"pass{h}"):
                    pass_down(h, row)

    list_cp = pltpu.make_async_remote_copy(
        src_ref=list_ref, dst_ref=plist_v, send_sem=list_sem.at[0], recv_sem=list_sem.at[1],
        device_id={"kv": partner}, device_id_type=MESH)

    def ranks(ref, ids, within):
        need = ids == ref[0, 0]
        for qb in range(nqb):
            for j in range(NSEL):
                need = need | (ids == ref[qb, j])
        need = need.astype(jnp.int32)
        rank = jnp.zeros_like(need)
        for d in range(1, nblk):
            rank = rank + jnp.where(within >= d, pltpu.roll(need, d, 1), 0)
        return need, rank

    def wanted(need, rank, within, owner):
        out = jnp.zeros((n, 128), jnp.int32)
        lane = lax.broadcasted_iota(jnp.int32, (n, 128), 1)
        here = owner == lax.broadcasted_iota(jnp.int32, (n, pos_v.shape[1]), 0)
        for k in range(cap):
            hit = here & (need == 1) & (rank == k)
            out = jnp.where(lane == k, jnp.sum(jnp.where(hit, within, 0), axis=1, keepdims=True), out)
        return out

    with jax.named_scope("fetch_first"):
        for f in range(PIECES):
            forward(0, 0, f)
        for cp in small_cp:
            cp.wait()
        list_cp.start()
        ids = lax.broadcasted_iota(jnp.int32, (1, pos_v.shape[1]), 1)
        owner = jnp.zeros_like(ids)
        for o in range(1, n):
            owner = owner + (ids >= o * nblk).astype(jnp.int32)
        within = ids - owner * nblk
        line = owner // 2
        own_col = owner - 2 * line == c
        need, rank = ranks(chosen_ref, ids, within)
        pos_v[nqb:nqb + 1, :] = jnp.where(own_col, line * nblk + within, compact + line * cap + rank)
        req_v[:n] = wanted(need, rank, within, owner)
        listed = list_ref[...]
        table_v[:nqb, :NSEL] = jnp.maximum(listed, 0)
        table_v[:nqb, NSEL:2 * NSEL] = jnp.where(listed >= 0, listed * BLK, 1 << 30)
        for qb in range(nqb):
            at = jnp.full(ids.shape, nqb * NSEL, jnp.int32)
            for j in range(NSEL):
                at = jnp.where(ids == chosen_ref[qb, j], qb * NSEL + j, at)
            pos_v[qb:qb + 1, :] = at
        for f in range(PIECES):
            forward(0, 1, f)
        list_cp.wait_recv()
        pch_v[:nqb, :NSEL] = plist_v[...]
        cp = pltpu.make_async_copy(pch_v, pch_ref, tab_sem.at[0])
        cp.start()
        cp.wait()
        need, rank = ranks(pch_ref, ids, within)
        pos_v[nqb + 1:nqb + 2, :] = jnp.where(need == 1, rank, cap)
        req_v[n:] = wanted(need, rank, within, owner)
        tab_cp = [
            pltpu.make_async_copy(table_v, table, tab_sem.at[0]),
            pltpu.make_async_copy(pos_v, pos_ref, tab_sem.at[1]),
            pltpu.make_async_copy(req_v, req_ref, tab_sem.at[2]),
        ]
        for cp in tab_cp:
            cp.start()
        for cp in tab_cp:
            cp.wait()
        across(0, 0)
        across(0, 1)
        w1[...] = jnp.zeros_like(w1)
        both_scr[nqb * NSEL] = jnp.zeros((BLK, 2 * DH), jnp.float32)
        for h in range(kv_heads):
            for row in range(rows_n):
                yrecv[h][row][cap] = jnp.zeros((BLK, 2 * DH), jnp.bfloat16)
        for qb in range(nqb):
            ls_t[qb] = ls_ref[:, qb * QB:(qb + 1) * QB]
        for k in range(2, rows_n):
            for f in range(PIECES):
                forward(0, k, f)
            across(0, k)
        for h in range(1, kv_heads):
            own_cp[h].wait()
            for f in range(PIECES):
                forward(h, 0, f)
            across(h, 0)
        arrived(0)
        for cp in in_cp:
            cp.wait()

    early = [nqb // 2 if h + 1 < kv_heads else 0 for h in range(kv_heads)]
    pieces = [(k, f) for k in range(1, rows_n) for f in range(PIECES)]
    dq_cp = []
    for h in range(kv_heads):
        def loop(qb, carry, h=h):
            with jax.named_scope(f"attend{h}"):
                attend(h, qb)
            if h + 1 < kv_heads:
                for i, (k, f) in enumerate(pieces):
                    @pl.when(qb == i * nqb // len(pieces))
                    def _():
                        with jax.named_scope("forward_next"):
                            forward(h + 1, k, f)
                            if f == PIECES - 1:
                                across(h + 1, k)
            if h > 0:
                for k in range(early[h - 1]):
                    @pl.when(qb == 2 * k + 1)
                    def _():
                        with jax.named_scope(f"ring{h - 1}"):
                            ring(h - 1, k + 1, False)
                        pass_slot(h - 1, k + 1 - OFFS[h - 1])
            return carry

        lax.fori_loop(0, nqb, loop, 0)
        dq_cp.append(pltpu.make_async_copy(
            dq_ref.at[:, h * width:(h + 1) * width], dq_hbm.at[:, h * width:(h + 1) * width], out_sem.at[h]))
        dq_cp[h].start()
        if h == 0:
            for cp in inp_cp:
                cp.wait()
        with jax.named_scope(f"ring_first{h}"):
            ring(h, 0, True)
        with jax.named_scope(f"give{h}"):
            give(h)
        if h + 1 < kv_heads:
            with jax.named_scope("arrive_next"):
                arrived(h + 1)

    kvg_cp = [pltpu.make_async_copy(
        kvg_ref.at[:, h * 2 * DH:(h + 1) * 2 * DH], kvg_hbm.at[:, h * 2 * DH:(h + 1) * 2 * DH],
        out_sem.at[kv_heads + h]) for h in range(kv_heads)]
    wg_cp = [pltpu.make_async_copy(
        wg_ref.at[:, h * width:(h + 1) * width], wg_hbm.at[:, h * width:(h + 1) * width],
        out_sem.at[2 * kv_heads + h]) for h in range(kv_heads)]

    def ring_loop(s, carry):
        for h in range(kv_heads):
            @pl.when(s + early[h] <= n - 2)
            def _():
                with jax.named_scope(f"ring{h}"):
                    ring(h, s + early[h], False)
            pass_slot(h, s + early[h] - OFFS[h])
            if early[h]:
                @pl.when(s == n - 2)
                def _():
                    with jax.named_scope(f"keep{h}"):
                        keep(h)
                    with jax.named_scope(f"ring_end{h}"):
                        ring_end(h)
        return carry

    lax.fori_loop(1, n - 1, ring_loop, 0)
    list_cp.wait_send()
    for h in range(kv_heads):
        for k in range(rows_n):
            if k < rows_n - 1:
                @pl.when((r >= k) & has_up)
                def _():
                    for f in range(PIECES):
                        zfetch(h, k, f).wait_send()

            @pl.when((r >= k) if k > 0 else (c == 0))
            def _():
                yfetch(h, k).wait_send()

        for row in range(rows_n):
            @pl.when(row < r + c)
            def _():
                gsend(h, row).wait_send()

            @pl.when(row < r)
            def _():
                zcopy(h, row).wait_send()

        def drain_r(s, carry, h=h):
            for u in range(SUBS):
                rcopy(h, u, s).wait_send()
            return carry

        lax.fori_loop(0, n - 2, drain_r, 0)
    for h in range(kv_heads):
        if not early[h]:
            with jax.named_scope(f"keep{h}"):
                keep(h)
            with jax.named_scope(f"ring_end{h}"):
                ring_end(h)
    for h in range(kv_heads):
        for u in range(SUBS):
            rcopy(h, u, n - 2).wait_send()
    for cp in dq_cp + kvg_cp + wg_cp:
        cp.wait()


def hand_on(*refs):
    srcs, dsts, bufs, sems = refs[:3], refs[3:6], refs[6:9], refs[9]
    pieces = []
    for i in range(3):
        step = srcs[i].shape[0] // 2
        for k in range(2):
            rows = slice(k * step, (k + 1) * step)
            pieces.append((
                pltpu.make_async_copy(srcs[i].at[rows], bufs[i].at[rows], sems.at[0, i, k]),
                pltpu.make_async_copy(bufs[i].at[rows], dsts[i].at[rows], sems.at[1, i, k])))
    for load, _ in pieces:
        load.start()
    for load, store in pieces:
        load.wait()
        store.start()
    for _, store in pieces:
        store.wait()


def shards(queries, keys_values, log_sums, out_grad, inputs, chosen):
    tok = queries.shape[0]
    heads_here = queries.shape[1] // DH
    kv_heads = keys_values.shape[1] // (2 * DH)
    group = heads_here // kv_heads
    nqb, nblk = tok // QB, tok // BLK
    n = lax.axis_size("kv")
    rows_n = n // 2
    row_width = keys_values.shape[1]
    cap = nblk // 2
    pos_w = pl.cdiv(n * nblk, 128) * 128
    lanes = group * QB
    width = group * DH
    sub_w = width // SUBS
    drow = inputs.shape[1] // n
    hbm = pl.BlockSpec(memory_space=pl.ANY)
    per_head = lambda shape, dtype: [pltpu.VMEM(shape, dtype)] * kv_heads
    bf, f32 = jnp.bfloat16, jnp.float32
    keys = NSEL * BLK
    dma = pltpu.SemaphoreType.DMA
    scratch = (
        per_head((rows_n * (nblk + cap), BLK, 2 * DH), bf)
        + per_head((nqb, width, QB), bf)
        + per_head((rows_n, nblk, BLK, 2 * DH), f32)
        + per_head((nblk, BLK, 2 * DH), bf) * rows_n
        + per_head((cap, BLK, 2 * DH), bf) * rows_n
        + per_head((rows_n, cap, BLK, 2 * DH), bf)
        + per_head((cap + 1, BLK, 2 * DH), bf) * rows_n
        + per_head((rows_n, nblk, BLK, 2 * DH), bf)
        + per_head((rows_n, nblk, BLK, 2 * DH), bf)
        + per_head((SUBS, n - 1, sub_w, drow), bf)
        + per_head((SUBS, n - 1, sub_w, drow), bf)
        + [
            pltpu.VMEM((n, tok, drow), bf),
            pltpu.VMEM((2 * DH, 2 * lanes), bf),
            pltpu.VMEM((keys, 2 * DH), bf),
            pltpu.VMEM((keys, lanes), f32),
            pltpu.VMEM((keys, lanes), f32),
            pltpu.VMEM((keys, 2 * lanes), bf),
            pltpu.VMEM((nqb * NSEL + 1, BLK, 2 * DH), f32),
            pltpu.VMEM((tok, heads_here * DH), bf),
            pltpu.VMEM((tok, heads_here * DH), bf),
            pltpu.VMEM((nqb, heads_here, QB), f32),
            pltpu.VMEM((tok, heads_here * DH), bf),
            pltpu.VMEM((tok, row_width), f32),
            pltpu.VMEM((drow, heads_here * DH), f32),
            pltpu.VMEM((8, 128), jnp.int32),
            pltpu.VMEM((8, pos_w), jnp.int32),
            pltpu.VMEM((2 * n, 128), jnp.int32),
            pltpu.VMEM((nqb, NSEL), jnp.int32),
            pltpu.VMEM((8, 128), jnp.int32),
            pltpu.SMEM((8, 128), jnp.int32),
            pltpu.SMEM((8, pos_w), jnp.int32),
            pltpu.SMEM((2 * n, 128), jnp.int32),
            pltpu.SMEM((8, 128), jnp.int32),
            pltpu.SMEM((nqb, NSEL), jnp.int32),
            pltpu.VMEM((nqb, NSEL), jnp.int32),
            pltpu.VMEM((heads_here, tok), f32),
            dma((n,)),
            dma((kv_heads,)),
            dma((5,)),
            dma((3,)),
            dma((3 * kv_heads,)),
            dma((2,)),
            dma((kv_heads, rows_n)),
            dma((kv_heads, PIECES, rows_n)),
            dma((kv_heads, rows_n)),
            dma((kv_heads, rows_n)),
            dma((kv_heads, PIECES, rows_n)),
            dma((kv_heads, rows_n)),
            dma((kv_heads, rows_n)),
            dma((kv_heads, rows_n)),
            dma((kv_heads, rows_n)),
            dma((kv_heads, SUBS, n - 1)),
            dma((kv_heads, SUBS, n - 1)),
        ]
    )
    shapes = [
        jax.ShapeDtypeStruct((tok, heads_here * DH), bf),
        jax.ShapeDtypeStruct((tok, row_width), f32),
        jax.ShapeDtypeStruct((drow, heads_here * DH), f32),
    ]
    raw = pl.pallas_call(
        functools.partial(whole, n, kv_heads, group, tok),
        in_specs=[hbm] * 6,
        out_specs=[hbm, hbm, hbm],
        out_shape=shapes,
        scratch_shapes=scratch,
        compiler_params=pltpu.CompilerParams(
            collective_id=0, has_side_effects=True, vmem_limit_bytes=63 * 1024 * 1024
        ),
    )(chosen, log_sums.T, queries, out_grad, keys_values.reshape(nblk, BLK, -1), inputs)
    return tuple(pl.pallas_call(
        hand_on,
        in_specs=[hbm] * 3,
        out_specs=[hbm] * 3,
        out_shape=shapes,
        scratch_shapes=[pltpu.VMEM(x.shape, x.dtype) for x in shapes] + [dma((2, 3, 2))],
    )(*raw))


def solution(mesh):
    in_specs = (
        P("kv", "tp"),
        P("kv", "tp"),
        P("kv", "tp"),
        P("kv", "tp"),
        P("kv", None),
        P("kv", None),
    )
    out_specs = (P("kv", "tp"), P("kv", "tp"), P("kv", "tp"))
    return jax.shard_map(shards, mesh=mesh, in_specs=in_specs, out_specs=out_specs, check_vma=False)
```

```python
import functools

import jax
import jax.numpy as jnp
from jax import lax
from jax.experimental import pallas as pl
from jax.experimental.pallas import tpu as pltpu
from jax.sharding import PartitionSpec as P

DH = 64
BLK = 64
QB = 128
NSEL = 16
CHUNK = 4
SCALE = DH ** (-0.5)
MESH = pl.DeviceIdType.MESH
SUBS = 4
PIECES = 2
PASS_EARLY = (1, 3)
PASS_LAST = (3, 1)


def whole(n, kv_heads, group, tok, chosen_hbm, ls_hbm, q_hbm, do_hbm, kv_hbm, inp_hbm,
          dq_hbm, kvg_hbm, wg_hbm, *scratch):
    it = iter(scratch)
    tabs = [next(it) for _ in range(kv_heads)]
    qts = [next(it) for _ in range(kv_heads)]
    owns = [next(it) for _ in range(kv_heads)]
    rows_n = n // 2
    arr = [[next(it) for _ in range(rows_n)] for _ in range(kv_heads)]
    stage = [[next(it) for _ in range(rows_n)] for _ in range(kv_heads)]
    ysend = [next(it) for _ in range(kv_heads)]
    yrecv = [[next(it) for _ in range(rows_n)] for _ in range(kv_heads)]
    zsend = [next(it) for _ in range(kv_heads)]
    zrecv = [next(it) for _ in range(kv_heads)]
    rsend = [next(it) for _ in range(kv_heads)]
    rrecv = [next(it) for _ in range(kv_heads)]
    inp, w1, kv_scr, p_scr, dp_scr, a_scr, both_scr = [next(it) for _ in range(7)]
    q_ref, do_ref, ls_t, dq_ref, kvg_ref, wg_ref, table_v, pos_v, req_v, plist_v, pch_v = [next(it) for _ in range(11)]
    table, pos_ref, req_ref, pch_ref, chosen_ref, list_ref, ls_ref = [next(it) for _ in range(7)]
    (inp_sem, own_sem, in_sem, tab_sem, out_sem, list_sem, loc_sem, fz_s, fy_s, fy_r, f_r, gy_s, gy_r, gz_s, gz_r, r_s, r_r) = [next(it) for _ in range(17)]

    nqb = tok // QB
    nblk = tok // BLK
    cap = nblk // 2
    blocks = n * nblk
    compact = rows_n * nblk
    lanes = group * QB
    width = group * DH
    sub_w = width // SUBS
    me = lax.axis_index("kv")
    r, c = me // 2, me % 2
    partner = 2 * r + 1 - c
    up, down = me + 2, me - 2
    has_up, has_down = r < rows_n - 1, r > 0

    def at_pos(p):
        p = lax.rem(p + 2 * n, n)
        return jnp.where(p < rows_n, 2 * p, 2 * (n - 1 - p) + 1)

    pos_me = jnp.where(c == 0, r, n - 1 - r)
    ring_to = (at_pos(pos_me + 1), at_pos(pos_me - 1))

    own_cp = [
        pltpu.make_async_copy(kv_hbm.at[:, :, h * 2 * DH:(h + 1) * 2 * DH], arr[h][0], own_sem.at[h])
        for h in range(kv_heads)
    ]
    small_cp = [
        pltpu.make_async_copy(chosen_hbm, list_ref, in_sem.at[2]),
        pltpu.make_async_copy(chosen_hbm, chosen_ref, in_sem.at[3]),
        pltpu.make_async_copy(ls_hbm, ls_ref, in_sem.at[4]),
    ]
    for cp in own_cp[:1] + small_cp + own_cp[1:]:
        cp.start()
    barrier = pltpu.get_barrier_semaphore()
    pl.semaphore_signal(barrier, inc=1, device_id={"kv": partner}, device_id_type=MESH)

    @pl.when(has_up)
    def _():
        pl.semaphore_signal(barrier, inc=1, device_id={"kv": up}, device_id_type=MESH)

    @pl.when(has_down)
    def _():
        pl.semaphore_signal(barrier, inc=1, device_id={"kv": down}, device_id_type=MESH)

    drow = inp_hbm.shape[1] // n
    inp_cp = [
        pltpu.make_async_copy(inp_hbm.at[:, i * drow:(i + 1) * drow], inp.at[i], inp_sem.at[i]) for i in range(n)
    ]
    in_cp = [
        pltpu.make_async_copy(q_hbm, q_ref, in_sem.at[0]),
        pltpu.make_async_copy(do_hbm, do_ref, in_sem.at[1]),
    ]
    for cp in in_cp:
        cp.start()
    for cp in inp_cp:
        cp.start()
    own_cp[0].wait()
    pl.semaphore_wait(barrier, 1 + has_up.astype(jnp.int32) + has_down.astype(jnp.int32))

    piece_n = nblk // PIECES

    def zfetch(h, k, f):
        src = arr[h][k].at[f * piece_n:(f + 1) * piece_n]
        dst = arr[h][min(k + 1, rows_n - 1)].at[f * piece_n:(f + 1) * piece_n]
        return pltpu.make_async_remote_copy(
            src_ref=src, dst_ref=dst, send_sem=fz_s.at[h, f, k], recv_sem=f_r.at[h, f, min(k + 1, rows_n - 1)],
            device_id={"kv": up}, device_id_type=MESH)

    def yfetch(h, k):
        return pltpu.make_async_remote_copy(
            src_ref=stage[h][k], dst_ref=tabs[h].at[pl.ds(compact + (r - k) * cap, cap)], send_sem=fy_s.at[h, k],
            recv_sem=fy_r.at[h, k], device_id={"kv": partner}, device_id_type=MESH)

    def local(h, k):
        return pltpu.make_async_copy(arr[h][k], tabs[h].at[pl.ds((r - k) * nblk, nblk)], loc_sem.at[h, k])

    def forward(h, k, f):
        @pl.when(r >= k)
        def _():
            if k > 0:
                zfetch(h, k - 1, f).wait_recv()
            if k < rows_n - 1:
                @pl.when(has_up)
                def _():
                    zfetch(h, k, f).start()

    def across(h, k):
        @pl.when(r >= k)
        def _():
            local(h, k).start()

            @pl.when((c == 0) if k == 0 else (c >= 0))
            def _():
                owner = 2 * (r - k) + c
                for i in range(cap):
                    stage[h][k][i] = arr[h][k][req_ref[n + owner, i]]
                yfetch(h, k).start()

    def arrived(h):
        for k in range(rows_n):
            @pl.when((r >= k) if k > 0 else (c == 1))
            def _():
                yfetch(h, k).wait_recv()

            @pl.when(r >= k)
            def _():
                local(h, k).wait()

    def attend(h, qb):
        tab = tabs[h]
        qrow = pl.ds(pl.multiple_of(qb * QB, QB), QB)
        cols = slice(h * width, (h + 1) * width)
        q_t = (q_ref[qrow, cols].astype(jnp.float32) * SCALE).T.astype(jnp.bfloat16)
        do_t = do_ref[qrow, cols].astype(jnp.float32).T.astype(jnp.bfloat16)
        for g in range(group):
            w1[:DH, g * QB:(g + 1) * QB] = q_t[g * DH:(g + 1) * DH]
            w1[DH:, lanes + g * QB:lanes + (g + 1) * QB] = do_t[g * DH:(g + 1) * DH]
        for j in range(NSEL):
            kv_scr[j * BLK:(j + 1) * BLK, :] = tab[pos_ref[nqb, table[qb, j]]]
        rows = CHUNK * BLK
        lane = lax.broadcasted_iota(jnp.int32, (1, lanes), 1)
        qpos = (me * nqb + qb) * QB + lax.rem(lane, QB)
        within = lax.broadcasted_iota(jnp.int32, (BLK, lanes), 0)
        sums = jnp.concatenate([ls_t[qb, h * group + g:h * group + g + 1, :] for g in range(group)], axis=1)
        delta = jnp.zeros((1, lanes), jnp.float32)
        for ch in range(NSEL // CHUNK):
            kv = kv_scr[ch * rows:(ch + 1) * rows, :]
            scores = jnp.dot(kv, w1[:, :lanes], preferred_element_type=jnp.float32)
            grads = jnp.dot(kv, w1[:, lanes:], preferred_element_type=jnp.float32)
            for i in range(CHUNK):
                last = qpos - table[qb, NSEL + ch * CHUNK + i]
                here = slice(i * BLK, (i + 1) * BLK)
                there = slice(ch * rows + i * BLK, ch * rows + (i + 1) * BLK)
                prob = jnp.where(within <= last, jnp.exp(scores[here] - sums), jnp.float32(0.0))
                rounded = prob.astype(jnp.bfloat16)
                delta += jnp.sum(rounded.astype(jnp.float32) * grads[here], axis=0, keepdims=True)
                p_scr[there, :] = prob
                dp_scr[there, :] = grads[here]
                a_scr[there, lanes:] = rounded
        for ch in range(NSEL // CHUNK):
            there = slice(ch * rows, (ch + 1) * rows)
            a_scr[there, :lanes] = (p_scr[there, :] * (dp_scr[there, :] - delta)).astype(jnp.bfloat16)
            both_scr[pl.ds(qb * NSEL + ch * CHUNK, CHUNK)] = lax.dot_general(
                a_scr[there, :], w1[...], (((1,), (1,)), ((), ())), preferred_element_type=jnp.float32
            ).reshape(CHUNK, BLK, 2 * DH)
        dq_t = jnp.dot(kv_scr[...].T, a_scr[:, :lanes], preferred_element_type=jnp.float32)[:DH] * SCALE
        stacked = jnp.concatenate([dq_t[:, g * QB:(g + 1) * QB] for g in range(group)], axis=0)
        qts[h][qb] = stacked.astype(jnp.bfloat16)
        dq_ref[qrow, cols] = stacked.T.astype(jnp.bfloat16)

    def block_sum(block):
        total = None
        for qb in range(nqb):
            part = both_scr[pos_ref[qb, block]]
            total = part if total is None else total + part
        return total

    def gsend(h, row):
        return pltpu.make_async_remote_copy(
            src_ref=ysend[h].at[row], dst_ref=yrecv[h][row].at[:cap], send_sem=gy_s.at[h, row],
            recv_sem=gy_r.at[h, row], device_id={"kv": partner}, device_id_type=MESH)

    def zcopy(h, row, f):
        part = pl.ds(f * piece_n, piece_n)
        return pltpu.make_async_remote_copy(
            src_ref=zsend[h].at[row, part], dst_ref=zrecv[h].at[row, part], send_sem=gz_s.at[h, f, row],
            recv_sem=gz_r.at[h, f, row], device_id={"kv": down}, device_id_type=MESH)

    def give(h):
        for row in range(rows_n):
            @pl.when(row < r + c)
            def _():
                def one(k, inner):
                    owner = 2 * row + 1 - c
                    ysend[h][row, k] = block_sum(owner * nblk + req_ref[owner, k]).astype(jnp.bfloat16)
                    return inner

                lax.fori_loop(0, cap, one, 0)
                gsend(h, row).start()

        def mine(i, carry):
            row, k = i // nblk, i % nblk
            owns[h][row, k] = block_sum((2 * row + c) * nblk + k)
            return carry

        lax.fori_loop(0, (r + 1) * nblk, mine, 0)

    def pass_down(h, row):
        gsend(h, row).wait_recv()

        def one(k, carry):
            total = owns[h][row, k] + yrecv[h][row][pos_ref[nqb + 1, (2 * row + c) * nblk + k]].astype(jnp.float32)

            @pl.when(has_up)
            def _():
                zsend[h][row, k] = (total + zrecv[h][row, k].astype(jnp.float32)).astype(jnp.bfloat16)

            @pl.when(jnp.logical_not(has_up))
            def _():
                zsend[h][row, k] = total.astype(jnp.bfloat16)

            return carry

        for f in range(PIECES):
            @pl.when(has_up)
            def _():
                zcopy(h, row, f).wait_recv()

            lax.fori_loop(f * piece_n, (f + 1) * piece_n, one, 0)
            zcopy(h, row, f).start()

    def keep(h):
        cols = slice(h * 2 * DH, (h + 1) * 2 * DH)

        @pl.when(has_up)
        def _():
            for f in range(PIECES):
                zcopy(h, r, f).wait_recv()
            kvg_ref[:, cols] = (owns[h][r] + zrecv[h][r].astype(jnp.float32)).reshape(tok, 2 * DH)

        @pl.when(jnp.logical_not(has_up))
        def _():
            kvg_ref[:, cols] = owns[h][r].reshape(tok, 2 * DH)

        for row in range(rows_n):
            @pl.when((c == 0) & (r == row))
            def _():
                gsend(h, row).wait_recv()
                for k in range(nblk):
                    kvg_ref[k * BLK:(k + 1) * BLK, cols] += (
                        yrecv[h][row][pos_ref[nqb + 1, (2 * row + c) * nblk + k]].astype(jnp.float32))

        kvg_cp[h].start()

    def rcopy(h, u, s):
        return pltpu.make_async_remote_copy(
            src_ref=rsend[h].at[u, s], dst_ref=rrecv[h].at[u, s], send_sem=r_s.at[h, u, s],
            recv_sem=r_r.at[h, u, s], device_id={"kv": ring_to[u * 2 // SUBS]}, device_id_type=MESH)

    half = width // 2

    def partial_of(h, d, target):
        chunk = inp[target]
        total = None
        for qb in range(nqb):
            part = jnp.dot(qts[h][qb, d * half:(d + 1) * half, :], chunk[qb * QB:(qb + 1) * QB, :],
                           preferred_element_type=jnp.float32)
            total = part if total is None else total + part
        return total

    def ring(h, s, first):
        parts = [partial_of(h, d, at_pos(pos_me - 1 - s) if d == 0 else at_pos(pos_me + 1 + s)) for d in range(2)]
        for v in range(SUBS // 2):
            for d in range(2):
                part = parts[d]
                u = d * (SUBS // 2) + v
                piece = part[v * sub_w:(v + 1) * sub_w]
                if not first:
                    rcopy(h, u, s - 1).wait_recv()
                    piece = piece + rrecv[h][u, s - 1].astype(jnp.float32)
                rsend[h][u, s] = piece.astype(jnp.bfloat16)
                rcopy(h, u, s).start()

    def ring_end(h):
        parts = [partial_of(h, d, me) for d in range(2)]
        for d in range(2):
            got = []
            for v in range(SUBS // 2):
                u = d * (SUBS // 2) + v
                rcopy(h, u, n - 2).wait_recv()
                got.append(parts[d][v * sub_w:(v + 1) * sub_w] + rrecv[h][u, n - 2].astype(jnp.float32))
            wg_ref[:, h * width + d * half:h * width + (d + 1) * half] = jnp.concatenate(got, axis=0).T
        wg_cp[h].start()

    def pass_slot(h, step):
        offset, skew = PASS_EARLY if early[h] else PASS_LAST
        skew = min(skew, (n - 2 + early[h] - offset) // max(rows_n - 2, 1))
        for row in range(rows_n - 1):
            @pl.when((step == offset + row + skew * (rows_n - 1 - r)) & (row < r))
            def _():
                with jax.named_scope(f"pass{h}"):
                    pass_down(h, row)

    list_cp = pltpu.make_async_remote_copy(
        src_ref=list_ref, dst_ref=plist_v, send_sem=list_sem.at[0], recv_sem=list_sem.at[1],
        device_id={"kv": partner}, device_id_type=MESH)

    def ranks(ref, ids, within):
        need = ids == ref[0, 0]
        for qb in range(nqb):
            for j in range(NSEL):
                need = need | (ids == ref[qb, j])
        need = need.astype(jnp.int32)
        rank = jnp.zeros_like(need)
        for d in range(1, nblk):
            rank = rank + jnp.where(within >= d, pltpu.roll(need, d, 1), 0)
        return need, rank

    def wanted(need, rank, within, owner):
        out = jnp.zeros((n, 128), jnp.int32)
        lane = lax.broadcasted_iota(jnp.int32, (n, 128), 1)
        here = owner == lax.broadcasted_iota(jnp.int32, (n, pos_v.shape[1]), 0)
        for k in range(cap):
            hit = here & (need == 1) & (rank == k)
            out = jnp.where(lane == k, jnp.sum(jnp.where(hit, within, 0), axis=1, keepdims=True), out)
        return out

    with jax.named_scope("fetch_first"):
        for f in range(PIECES):
            forward(0, 0, f)
        for cp in small_cp:
            cp.wait()
        list_cp.start()
        ids = lax.broadcasted_iota(jnp.int32, (1, pos_v.shape[1]), 1)
        owner = jnp.zeros_like(ids)
        for o in range(1, n):
            owner = owner + (ids >= o * nblk).astype(jnp.int32)
        within = ids - owner * nblk
        line = owner // 2
        own_col = owner - 2 * line == c
        need, rank = ranks(chosen_ref, ids, within)
        pos_v[nqb:nqb + 1, :] = jnp.where(own_col, line * nblk + within, compact + line * cap + rank)
        req_v[:n] = wanted(need, rank, within, owner)
        listed = list_ref[...]
        table_v[:nqb, :NSEL] = jnp.maximum(listed, 0)
        table_v[:nqb, NSEL:2 * NSEL] = jnp.where(listed >= 0, listed * BLK, 1 << 30)
        for qb in range(nqb):
            at = jnp.full(ids.shape, nqb * NSEL, jnp.int32)
            for j in range(NSEL):
                at = jnp.where(ids == chosen_ref[qb, j], qb * NSEL + j, at)
            pos_v[qb:qb + 1, :] = at
        for f in range(PIECES):
            forward(0, 1, f)
        list_cp.wait_recv()
        pch_v[:nqb, :NSEL] = plist_v[...]
        cp = pltpu.make_async_copy(pch_v, pch_ref, tab_sem.at[0])
        cp.start()
        cp.wait()
        need, rank = ranks(pch_ref, ids, within)
        pos_v[nqb + 1:nqb + 2, :] = jnp.where(need == 1, rank, cap)
        req_v[n:] = wanted(need, rank, within, owner)
        tab_cp = [
            pltpu.make_async_copy(table_v, table, tab_sem.at[0]),
            pltpu.make_async_copy(pos_v, pos_ref, tab_sem.at[1]),
            pltpu.make_async_copy(req_v, req_ref, tab_sem.at[2]),
        ]
        for cp in tab_cp:
            cp.start()
        for cp in tab_cp:
            cp.wait()
        across(0, 0)
        across(0, 1)
        w1[...] = jnp.zeros_like(w1)
        both_scr[nqb * NSEL] = jnp.zeros((BLK, 2 * DH), jnp.float32)
        for h in range(kv_heads):
            for row in range(rows_n):
                yrecv[h][row][cap] = jnp.zeros((BLK, 2 * DH), jnp.bfloat16)
        for qb in range(nqb):
            ls_t[qb] = ls_ref[:, qb * QB:(qb + 1) * QB]
        for k in range(2, rows_n):
            for f in range(PIECES):
                forward(0, k, f)
            across(0, k)
        for h in range(1, kv_heads):
            own_cp[h].wait()
            for f in range(PIECES):
                forward(h, 0, f)
            across(h, 0)
        arrived(0)
        for cp in in_cp:
            cp.wait()

    early = [nqb // 2 if h + 1 < kv_heads else 0 for h in range(kv_heads)]
    pieces = [(k, f) for k in range(1, rows_n) for f in range(PIECES)]
    dq_cp = []
    for h in range(kv_heads):
        def loop(qb, carry, h=h):
            with jax.named_scope(f"attend{h}"):
                attend(h, qb)
            if h + 1 < kv_heads:
                for i, (k, f) in enumerate(pieces):
                    @pl.when(qb == i * nqb // len(pieces))
                    def _():
                        with jax.named_scope("forward_next"):
                            forward(h + 1, k, f)
                            if f == PIECES - 1:
                                across(h + 1, k)
            if h > 0:
                for k in range(early[h - 1]):
                    @pl.when(qb == 2 * k + 1)
                    def _():
                        with jax.named_scope(f"ring{h - 1}"):
                            ring(h - 1, k + 1, False)
                        pass_slot(h - 1, k + 1)
            return carry

        lax.fori_loop(0, nqb, loop, 0)
        dq_cp.append(pltpu.make_async_copy(
            dq_ref.at[:, h * width:(h + 1) * width], dq_hbm.at[:, h * width:(h + 1) * width], out_sem.at[h]))
        dq_cp[h].start()
        if h == 0:
            for cp in inp_cp:
                cp.wait()
        with jax.named_scope(f"ring_first{h}"):
            ring(h, 0, True)
        with jax.named_scope(f"give{h}"):
            give(h)
        if h + 1 < kv_heads:
            with jax.named_scope("arrive_next"):
                arrived(h + 1)

    kvg_cp = [pltpu.make_async_copy(
        kvg_ref.at[:, h * 2 * DH:(h + 1) * 2 * DH], kvg_hbm.at[:, h * 2 * DH:(h + 1) * 2 * DH],
        out_sem.at[kv_heads + h]) for h in range(kv_heads)]
    wg_cp = [pltpu.make_async_copy(
        wg_ref.at[:, h * width:(h + 1) * width], wg_hbm.at[:, h * width:(h + 1) * width],
        out_sem.at[2 * kv_heads + h]) for h in range(kv_heads)]

    def ring_loop(s, carry):
        for h in range(kv_heads):
            @pl.when(s + early[h] <= n - 2)
            def _():
                with jax.named_scope(f"ring{h}"):
                    ring(h, s + early[h], False)
            pass_slot(h, s + early[h])
            if early[h]:
                @pl.when(s == n - 2)
                def _():
                    with jax.named_scope(f"keep{h}"):
                        keep(h)
                    with jax.named_scope(f"ring_end{h}"):
                        ring_end(h)
        return carry

    lax.fori_loop(1, n - 1, ring_loop, 0)
    list_cp.wait_send()
    for h in range(kv_heads):
        for k in range(rows_n):
            if k < rows_n - 1:
                @pl.when((r >= k) & has_up)
                def _():
                    for f in range(PIECES):
                        zfetch(h, k, f).wait_send()

            @pl.when((r >= k) if k > 0 else (c == 0))
            def _():
                yfetch(h, k).wait_send()

        for row in range(rows_n):
            @pl.when(row < r + c)
            def _():
                gsend(h, row).wait_send()

            @pl.when(row < r)
            def _():
                for f in range(PIECES):
                    zcopy(h, row, f).wait_send()

        def drain_r(s, carry, h=h):
            for u in range(SUBS):
                rcopy(h, u, s).wait_send()
            return carry

        lax.fori_loop(0, n - 2, drain_r, 0)
    for h in range(kv_heads):
        if not early[h]:
            with jax.named_scope(f"ring_end{h}"):
                ring_end(h)
            with jax.named_scope(f"keep{h}"):
                keep(h)
    for h in range(kv_heads):
        for u in range(SUBS):
            rcopy(h, u, n - 2).wait_send()
    for cp in dq_cp + kvg_cp + wg_cp:
        cp.wait()


def hand_on(*refs):
    srcs, dsts, bufs, sems = refs[:3], refs[3:6], refs[6:9], refs[9]
    pieces = []
    for i in range(3):
        step = srcs[i].shape[0] // 2
        for k in range(2):
            rows = slice(k * step, (k + 1) * step)
            pieces.append((
                pltpu.make_async_copy(srcs[i].at[rows], bufs[i].at[rows], sems.at[0, i, k]),
                pltpu.make_async_copy(bufs[i].at[rows], dsts[i].at[rows], sems.at[1, i, k])))
    for load, _ in pieces:
        load.start()
    for load, store in pieces:
        load.wait()
        store.start()
    for _, store in pieces:
        store.wait()


def shards(queries, keys_values, log_sums, out_grad, inputs, chosen):
    tok = queries.shape[0]
    heads_here = queries.shape[1] // DH
    kv_heads = keys_values.shape[1] // (2 * DH)
    group = heads_here // kv_heads
    nqb, nblk = tok // QB, tok // BLK
    n = lax.axis_size("kv")
    rows_n = n // 2
    row_width = keys_values.shape[1]
    cap = nblk // 2
    pos_w = pl.cdiv(n * nblk, 128) * 128
    lanes = group * QB
    width = group * DH
    sub_w = width // SUBS
    drow = inputs.shape[1] // n
    hbm = pl.BlockSpec(memory_space=pl.ANY)
    per_head = lambda shape, dtype: [pltpu.VMEM(shape, dtype)] * kv_heads
    bf, f32 = jnp.bfloat16, jnp.float32
    keys = NSEL * BLK
    dma = pltpu.SemaphoreType.DMA
    scratch = (
        per_head((rows_n * (nblk + cap), BLK, 2 * DH), bf)
        + per_head((nqb, width, QB), bf)
        + per_head((rows_n, nblk, BLK, 2 * DH), f32)
        + per_head((nblk, BLK, 2 * DH), bf) * rows_n
        + per_head((cap, BLK, 2 * DH), bf) * rows_n
        + per_head((rows_n, cap, BLK, 2 * DH), bf)
        + per_head((cap + 1, BLK, 2 * DH), bf) * rows_n
        + per_head((rows_n, nblk, BLK, 2 * DH), bf)
        + per_head((rows_n, nblk, BLK, 2 * DH), bf)
        + per_head((SUBS, n - 1, sub_w, drow), bf)
        + per_head((SUBS, n - 1, sub_w, drow), bf)
        + [
            pltpu.VMEM((n, tok, drow), bf),
            pltpu.VMEM((2 * DH, 2 * lanes), bf),
            pltpu.VMEM((keys, 2 * DH), bf),
            pltpu.VMEM((keys, lanes), f32),
            pltpu.VMEM((keys, lanes), f32),
            pltpu.VMEM((keys, 2 * lanes), bf),
            pltpu.VMEM((nqb * NSEL + 1, BLK, 2 * DH), f32),
            pltpu.VMEM((tok, heads_here * DH), bf),
            pltpu.VMEM((tok, heads_here * DH), bf),
            pltpu.VMEM((nqb, heads_here, QB), f32),
            pltpu.VMEM((tok, heads_here * DH), bf),
            pltpu.VMEM((tok, row_width), f32),
            pltpu.VMEM((drow, heads_here * DH), f32),
            pltpu.VMEM((8, 128), jnp.int32),
            pltpu.VMEM((8, pos_w), jnp.int32),
            pltpu.VMEM((2 * n, 128), jnp.int32),
            pltpu.VMEM((nqb, NSEL), jnp.int32),
            pltpu.VMEM((8, 128), jnp.int32),
            pltpu.SMEM((8, 128), jnp.int32),
            pltpu.SMEM((8, pos_w), jnp.int32),
            pltpu.SMEM((2 * n, 128), jnp.int32),
            pltpu.SMEM((8, 128), jnp.int32),
            pltpu.SMEM((nqb, NSEL), jnp.int32),
            pltpu.VMEM((nqb, NSEL), jnp.int32),
            pltpu.VMEM((heads_here, tok), f32),
            dma((n,)),
            dma((kv_heads,)),
            dma((5,)),
            dma((3,)),
            dma((3 * kv_heads,)),
            dma((2,)),
            dma((kv_heads, rows_n)),
            dma((kv_heads, PIECES, rows_n)),
            dma((kv_heads, rows_n)),
            dma((kv_heads, rows_n)),
            dma((kv_heads, PIECES, rows_n)),
            dma((kv_heads, rows_n)),
            dma((kv_heads, rows_n)),
            dma((kv_heads, PIECES, rows_n)),
            dma((kv_heads, PIECES, rows_n)),
            dma((kv_heads, SUBS, n - 1)),
            dma((kv_heads, SUBS, n - 1)),
        ]
    )
    shapes = [
        jax.ShapeDtypeStruct((tok, heads_here * DH), bf),
        jax.ShapeDtypeStruct((tok, row_width), f32),
        jax.ShapeDtypeStruct((drow, heads_here * DH), f32),
    ]
    raw = pl.pallas_call(
        functools.partial(whole, n, kv_heads, group, tok),
        in_specs=[hbm] * 6,
        out_specs=[hbm, hbm, hbm],
        out_shape=shapes,
        scratch_shapes=scratch,
        compiler_params=pltpu.CompilerParams(
            collective_id=0, has_side_effects=True, vmem_limit_bytes=63 * 1024 * 1024
        ),
    )(chosen, log_sums.T, queries, out_grad, keys_values.reshape(nblk, BLK, -1), inputs)
    return tuple(pl.pallas_call(
        hand_on,
        in_specs=[hbm] * 3,
        out_specs=[hbm] * 3,
        out_shape=shapes,
        scratch_shapes=[pltpu.VMEM(x.shape, x.dtype) for x in shapes] + [dma((2, 3, 2))],
    )(*raw))


def solution(mesh):
    in_specs = (
        P("kv", "tp"),
        P("kv", "tp"),
        P("kv", "tp"),
        P("kv", "tp"),
        P("kv", None),
        P("kv", None),
    )
    out_specs = (P("kv", "tp"), P("kv", "tp"), P("kv", "tp"))
    return jax.shard_map(shards, mesh=mesh, in_specs=in_specs, out_specs=out_specs, check_vma=False)
```
